32 devices in a mesh: ep: 8 (over z, y), tp: 4 (over x, core).
Axes of the slice: x: 2, y: 2, z: 4, core: 2. Of those that a mesh axis runs over, the one named last changes fastest.
Arguments:
- hidden: bfloat16 [256, 2048], P('ep')
- norm_gains: float32 [4, 2048], replicated, may hold values from 0.1 to 1.9
- w_query: bfloat16 [2048, 1024], P(None, 'tp'), may hold values from -0.125 to 0.125
- w_key: bfloat16 [2048, 1024], P(None, 'tp'), may hold values from -0.125 to 0.125
- w_value: bfloat16 [2048, 1024], P(None, 'tp'), may hold values from -0.125 to 0.125
- w_outgate: bfloat16 [2048, 1024], P(None, 'tp'), may hold values from -0.125 to 0.125
- w_input_gate: bfloat16 [2048, 8], replicated, may hold values from -0.125 to 0.125
- w_forget_gate: bfloat16 [2048, 8], replicated, may hold values from -0.125 to 0.125
- forget_bias: float32 [8], replicated, may hold values from -1 to 4
- w_mix_out: bfloat16 [1024, 2048], P('tp')
- state_matrix: float32 [256, 8, 128, 128], P('ep', 'tp'), may hold values from -0.6 to 0.6
- state_norm: float32 [256, 8, 128], P('ep', 'tp'), may hold values from -0.6 to 0.6
- state_max: float32 [256, 8], P('ep', 'tp'), may hold values from -4 to 4
- routes: int32 [256, 2], P('ep'), may hold values from 0 to 7, all different within a row; in each aligned block of 32 rows (0 to 31, 32 to 63, ...) at most 16 rows name the same one
- route_scores: float32 [256, 2], P('ep'), may hold values from 0.1 to 1
- expert_gate: bfloat16 [8, 2048, 3584], P('ep', None, 'tp'), may hold values from -0.125 to 0.125
- expert_up: bfloat16 [8, 2048, 3584], P('ep', None, 'tp'), may hold values from -0.125 to 0.125
- expert_down: bfloat16 [8, 3584, 2048], P('ep', 'tp')
- dense_gate: bfloat16 [2048, 5632], P('tp', 'ep'), may hold values from -0.125 to 0.125
- dense_up: bfloat16 [2048, 5632], P('tp', 'ep'), may hold values from -0.125 to 0.125
- dense_down: bfloat16 [5632, 2048], P('ep', 'tp')
- dense_mix: float32 [2048], replicated, may hold values from -0.25 to 0.25
Outputs:
- new_hidden: bfloat16 [256, 2048], P('ep', 'tp')
- new_matrix: float32 [256, 8, 128, 128], P('ep', 'tp')
- new_norm: float32 [256, 8, 128], P('ep', 'tp')
- new_max: float32 [256, 8], P('ep', 'tp')
The draws below stay inside these ranges and needn't reach their ends.
Inputs may be any that keep to these rules, and one draw needn't show every extreme that they name: `routes`: each row names 2 different experts. Among the rows of one index of ep (an aligned block of 32 rows) no expert is named by more than 16 rows, and in every draw some expert is named by exactly 16 rows of some block.
All inputs are finite; a program needn't handle non-finite values.
Results may differ from the reference program's by a relative error of at most 0.02.
Values may be sent and summed in bfloat16 or wider, within the bound.
A program may use at most 128 MiB of HBM per device.

```python
import math
import jax
import jax.numpy as jnp
import numpy as np
from jax import lax

D = 2048
HEADS = 8
HEAD = 128
FF_E = 3584
FF = 5632
TOP = 2
SEQ_DEV = 32
EXPERTS = 8
CAP = 16
SEQS = 256
N_EP = 8
N_TP = 4


def column_scaled(key, array_shape, fan_in, marker):
    noise_key, level_key = jax.random.split(jax.random.fold_in(key, marker))
    columns = array_shape[-1]
    position = jnp.arange(columns, dtype=jnp.float32) / columns
    levels = 0.5 * position + 0.5 * jax.random.uniform(level_key, (columns,), jnp.float32)
    noise = jax.random.normal(noise_key, array_shape, jnp.float32)
    scales = 10.0 ** levels
    scales = scales / jnp.sqrt(jnp.mean(scales * scales))
    return (noise * scales * (1.0 / fan_in) ** 0.5).astype(jnp.bfloat16)


def draw_hidden(key, part):
    return column_scaled(key, (SEQS, D), 1, 101)


def draw_w_mix_out(key, part):
    return column_scaled(key, (HEADS * HEAD, D), HEADS * HEAD, 102)


def draw_expert_down(key, part):
    return column_scaled(key, (EXPERTS, FF_E, D), FF_E, 103)


def draw_dense_down(key, part):
    return column_scaled(key, (FF, D), FF, 104)


def block_levels(rng, shape, cuts, low, top_value):
    gain = 1.0
    for axis_at, parts in cuts:
        heights = jax.random.uniform(jax.random.fold_in(jax.random.fold_in(rng, 6), axis_at), (parts,), jnp.float32, low / len(cuts), top_value / len(cuts))
        gain = gain * jnp.repeat(jnp.exp(heights), shape[axis_at] // parts).reshape((-1,) + (1,) * (len(shape) - 1 - axis_at))
    return gain


def deal_out(own_key, own, number, rows, amount, top, limit, lean):
    order = jax.random.permutation(own_key, amount)
    heavy_load, ordinary = load_shares(amount, rows * top, limit, lean, True), load_shares(amount, rows * top, limit, lean, False)
    places = jnp.arange(amount)

    def named(tallies, rotation):
        used = int((tallies > 0).sum())
        fixed = max(1, used // 4)
        passed = fixed + (places - fixed + rotation * (used - fixed)) % max(1, amount - fixed)
        return jnp.zeros((amount,), jnp.int32).at[order[jnp.where(places < fixed, places, passed)]].set(jnp.asarray(tallies, jnp.int32))

    tallies = jnp.where(number % 4 == 0, named(heavy_load, number // 4), named(ordinary, number - number // 4 - 1))
    mixed = jax.random.permutation(jax.random.fold_in(own, 3), amount)
    giver, sink = mixed[0:amount // 2 * 2:2], mixed[1:amount // 2 * 2:2]
    slack = jnp.minimum(tallies[giver] - 1, limit - tallies[sink]) // 2
    slack = jnp.where((giver == order[0]) | (sink == order[0]) | (tallies[sink] == 0), 0, jnp.maximum(slack, 0))
    passed = jax.random.randint(jax.random.fold_in(own, 4), (amount // 2,), 0, 1 << 20) % (slack + 1)
    tallies = tallies.at[giver].add(-passed).at[sink].add(passed)
    members = jnp.searchsorted(jnp.cumsum(tallies), jnp.arange(rows * top), side="right").astype(jnp.int32)
    table = members.reshape(top, rows).T
    table = table[jax.random.permutation(jax.random.fold_in(own, 1), rows)]
    rotation = jax.random.randint(jax.random.fold_in(own, 2), (rows, 1), 0, top)
    return jnp.take_along_axis(table, (jnp.arange(top)[None, :] + rotation) % top, axis=1)


def load_shares(number_of, total, most, lean, full):
    portions = [(1 << 20) // math.isqrt(standing ** lean) + 1 for standing in range(1, number_of + 1)]
    largest = most if full else min(most, max(-(-total // number_of), total * portions[0] // sum(portions)))
    least = 1 if total - largest >= number_of - 1 else 0
    counts, surplus = [largest] + [least] * (number_of - 1), total - largest - least * (number_of - 1)
    while surplus > 0:
        candidates = [i for i in range(1, number_of) if counts[i] < largest] or [i for i in range(1, number_of) if counts[i] < most]
        pool, left = sum([portions[i] for i in candidates]), surplus
        for i in candidates:
            extra = min(most - counts[i], max(1, left * portions[i] // pool), surplus)
            counts[i] = counts[i] + extra
            surplus = surplus - extra
    return np.array(counts)


def normal_values(rng, dims, deviation, reach, shards=(), held_as=jnp.bfloat16):
    values = jax.random.normal(rng, dims, jnp.float32) * deviation
    if len(shards) > 0:
        values = block_levels(rng, dims, shards, -0.22, 0.18) * values
    return jnp.clip(values, min=-reach, max=reach).astype(held_as)


def setup_inputs(seed: int = 0) -> dict:
    arg_keys = jax.random.split(jax.random.key(seed), 23)
    hidden = draw_hidden(jax.random.fold_in(arg_keys[22], 71), 0)
    norm_gains = jnp.clip(1.0 + 0.18 * jax.random.normal(arg_keys[1], (4, D), jnp.float32), 0.1, 1.9)
    w_query = normal_values(arg_keys[2], (D, HEADS * HEAD), D ** -0.5, 0.125, ((1, 4),))
    w_key = normal_values(arg_keys[3], (D, HEADS * HEAD), D ** -0.5, 0.125, ((1, 4),))
    w_value = normal_values(arg_keys[4], (D, HEADS * HEAD), D ** -0.5, 0.125, ((1, 4),))
    w_outgate = normal_values(arg_keys[5], (D, HEADS * HEAD), D ** -0.5, 0.125, ((1, 4),))
    w_input_gate = normal_values(arg_keys[6], (D, HEADS), D ** -0.5, 0.125)
    w_forget_gate = normal_values(arg_keys[7], (D, HEADS), D ** -0.5, 0.125)
    forget_bias = jnp.clip(jax.random.uniform(arg_keys[8], (HEADS,), jnp.float32, -1.0, 4.0), -1.0, 4.0)
    w_mix_out = draw_w_mix_out(jax.random.fold_in(arg_keys[22], 71), 0)
    state_matrix = normal_values(arg_keys[10], (SEQS, HEADS, HEAD, HEAD), 0.1, 0.6, ((0, 8), (1, 4)), jnp.float32)
    state_norm = normal_values(arg_keys[11], (SEQS, HEADS, HEAD), 0.1, 0.6, ((0, 8), (1, 4)), jnp.float32)
    state_max = normal_values(arg_keys[12], (SEQS, HEADS), 1.0, 4.0, ((0, 8), (1, 4)), jnp.float32)
    routes_keys = jax.random.split(jax.random.fold_in(arg_keys[13], 1), SEQS // SEQ_DEV)
    routes_turns = jax.random.permutation(jax.random.fold_in(arg_keys[13], 3), SEQS // SEQ_DEV)
    routes = jax.vmap(lambda own, number: deal_out(jax.random.fold_in(arg_keys[13], 2), own, number, SEQ_DEV, EXPERTS, TOP, CAP, 2))(routes_keys, routes_turns).reshape((SEQS, TOP))
    route_scores = jnp.clip(jnp.exp(math.log(1.0) - 2.3025851 * jax.random.uniform(arg_keys[14], (SEQS, TOP), jnp.float32) ** block_levels(arg_keys[14], (SEQS, TOP), ((0, 8),), -0.2, 0.2)), 0.1, 1.0)
    expert_gate = normal_values(arg_keys[15], (EXPERTS, D, FF_E), D ** -0.5, 0.125, ((0, 8), (2, 4)))
    expert_up = normal_values(arg_keys[16], (EXPERTS, D, FF_E), D ** -0.5, 0.125, ((0, 8), (2, 4)))
    expert_down = draw_expert_down(jax.random.fold_in(arg_keys[22], 71), 0)
    dense_gate = normal_values(arg_keys[18], (D, FF), D ** -0.5, 0.125, ((0, 4), (1, 8)))
    dense_up = normal_values(arg_keys[19], (D, FF), D ** -0.5, 0.125, ((0, 4), (1, 8)))
    dense_down = draw_dense_down(jax.random.fold_in(arg_keys[22], 71), 0)
    dense_mix = normal_values(arg_keys[21], (D,), (D // 4) ** -0.5, 0.25, (), jnp.float32)
    return dict(hidden=hidden, norm_gains=norm_gains, w_query=w_query, w_key=w_key, w_value=w_value, w_outgate=w_outgate, w_input_gate=w_input_gate, w_forget_gate=w_forget_gate, forget_bias=forget_bias, w_mix_out=w_mix_out, state_matrix=state_matrix, state_norm=state_norm, state_max=state_max, routes=routes, route_scores=route_scores, expert_gate=expert_gate, expert_up=expert_up, expert_down=expert_down, dense_gate=dense_gate, dense_up=dense_up, dense_down=dense_down, dense_mix=dense_mix)


EPS = 1e-06

def inverse_rms(values):
    return lax.rsqrt(lax.optimization_barrier(jnp.mean(values * values, axis=-1, keepdims=True)) + EPS)

def settle(values):
    return lax.optimization_barrier(values.astype(jnp.bfloat16)).astype(jnp.float32)

def grouped_product(activations, weights_in):
    row_count, inner_width = activations.shape
    group_width = inner_width // N_TP
    left_side = activations.astype(jnp.float32).reshape(row_count, N_TP, group_width)
    right_side = weights_in.astype(jnp.float32).reshape(N_TP, group_width, weights_in.shape[1])
    pieces = settle(jnp.einsum('rbf,bfd->brd', left_side, right_side))
    return lax.optimization_barrier(jnp.sum(pieces, axis=0)).astype(jnp.bfloat16)

def reference(hidden, norm_gains, w_query, w_key, w_value, w_outgate, w_input_gate, w_forget_gate, forget_bias, w_mix_out, state_matrix, state_norm, state_max, routes, route_scores, expert_gate, expert_up, expert_down, dense_gate, dense_up, dense_down, dense_mix):
    start_f = hidden.astype(jnp.float32)
    normed_in = (start_f * inverse_rms(start_f) * norm_gains[0]).astype(jnp.bfloat16)

    def project(weight):
        return settle(jnp.dot(normed_in, weight, preferred_element_type=jnp.float32))
    query = project(w_query).reshape(SEQS, HEADS, HEAD)
    keys = project(w_key).reshape(SEQS, HEADS, HEAD) * HEAD ** (-0.5)
    values = project(w_value).reshape(SEQS, HEADS, HEAD)
    out_gate = project(w_outgate)
    in_gate = jnp.dot(normed_in, w_input_gate, preferred_element_type=jnp.float32)
    log_forget = jax.nn.log_sigmoid(jnp.dot(normed_in, w_forget_gate, preferred_element_type=jnp.float32) + forget_bias)
    carried = log_forget + state_max
    new_max = jnp.maximum(carried, in_gate)
    keep = jnp.exp(carried - new_max)
    write = jnp.exp(in_gate - new_max)
    written = write[:, :, None] * keys
    new_matrix = keep[:, :, None, None] * state_matrix + written[:, :, :, None] * values[:, :, None, :]
    new_norm = keep[:, :, None] * state_norm + written
    numer = jnp.einsum('shd,shdv->shv', query, new_matrix)
    denom = jnp.einsum('shd,shd->sh', query, new_norm)
    read = numer / jnp.maximum(jnp.abs(denom), jnp.exp(-new_max))[:, :, None]
    mixed = (jax.nn.sigmoid(out_gate) * read.reshape(SEQS, HEADS * HEAD)).astype(jnp.bfloat16)
    branch = settle(grouped_product(mixed, w_mix_out))
    residual_f = start_f + norm_gains[1] * branch * inverse_rms(branch)
    residual = settle(residual_f)
    scale_two = inverse_rms(residual_f)
    normed = (residual_f * scale_two * norm_gains[2]).astype(jnp.bfloat16)
    mix_gate = jax.nn.sigmoid(scale_two[:, 0] * lax.optimization_barrier(jnp.sum(residual_f * norm_gains[2] * dense_mix, axis=-1)))
    dense_pre_gate = jnp.dot(normed, dense_gate, preferred_element_type=jnp.float32)
    dense_pre_up = jnp.dot(normed, dense_up, preferred_element_type=jnp.float32)
    dense_hidden = (jax.nn.silu(dense_pre_gate) * dense_pre_up).astype(jnp.bfloat16)
    dense_out = jnp.dot(dense_hidden, dense_down, preferred_element_type=jnp.float32)
    pairs = routes.reshape(N_EP, SEQ_DEV * TOP).astype(jnp.int32)
    picks = (pairs[:, :, None] == jnp.arange(EXPERTS, dtype=jnp.int32)[None, None, :]).astype(jnp.int32)
    ranks = (lax.optimization_barrier(jnp.sum(jnp.cumsum(picks, axis=1) * picks, axis=-1)) - 1).astype(jnp.int32)
    buffer_row = (jnp.arange(N_EP, dtype=jnp.int32)[:, None] * CAP + ranks).reshape(-1).astype(jnp.int32)
    flat_expert = pairs.reshape(-1)
    token_index = (jnp.arange(SEQS * TOP, dtype=jnp.int32) // TOP).astype(jnp.int32)
    expert_in = jnp.zeros((EXPERTS, N_EP * CAP, D), jnp.bfloat16).at[flat_expert, buffer_row].set(normed[token_index])

    def run_expert(operands):
        inputs, gate_weight, up_weight, down_weight = operands
        gate_pre = jnp.dot(inputs, gate_weight, preferred_element_type=jnp.float32)
        up_pre = jnp.dot(inputs, up_weight, preferred_element_type=jnp.float32)
        hidden_units = (jax.nn.silu(gate_pre) * up_pre).astype(jnp.bfloat16)
        return grouped_product(hidden_units, down_weight)
    expert_out = lax.map(run_expert, (expert_in, expert_gate, expert_up, expert_down))
    picked = settle(expert_out[flat_expert, buffer_row]).reshape(SEQS, TOP, D)
    share = route_scores / lax.optimization_barrier(jnp.sum(route_scores, axis=-1, keepdims=True))
    ffn = lax.optimization_barrier(jnp.sum(share[:, :, None] * picked, axis=1)) + mix_gate[:, None] * dense_out
    new_hidden = (residual + norm_gains[3] * ffn * inverse_rms(ffn)).astype(jnp.bfloat16)
    return (new_hidden, new_matrix, new_norm, new_max)
```

```python
import functools

import jax
import jax.numpy as jnp
from jax import lax
from jax.experimental import pallas as pl
from jax.experimental.pallas import tpu as pltpu
from jax.sharding import PartitionSpec as P

EPS = 1e-06


def front_kernel(
    hidden_ref,
    gains_ref,
    in_ref,
    forget_ref,
    bias_ref,
    norm_ref,
    max_ref,
    wq_hbm,
    wk_hbm,
    wv_hbm,
    wo_hbm,
    wm_hbm,
    state_hbm,
    terms_ref,
    matrix_hbm,
    new_norm_ref,
    new_max_ref,
    wq,
    wk,
    wv,
    wo,
    wm,
    state,
    numer,
    w_sem,
    in_sem,
    out_sem,
):
    tp = lax.axis_index("tp")
    f32, bf16 = jnp.float32, jnp.bfloat16
    seqs = hidden_ref.shape[0]
    heads, head = state.shape[1], state.shape[2]
    chunks = in_sem.shape[0]
    step = seqs // chunks
    loads = []
    for i, (src, dst) in enumerate(((wk_hbm, wk), (wq_hbm, wq), (wv_hbm, wv), (wo_hbm, wo))):
        loads.append(pltpu.make_async_copy(src, dst, w_sem.at[i]))
        loads[i].start()
    fetches = []
    for c in range(chunks):
        rows = pl.ds(c * step, step)
        fetches.append(pltpu.make_async_copy(state_hbm.at[rows], state.at[rows], in_sem.at[c]))
        fetches[c].start()
    loads.append(pltpu.make_async_copy(wm_hbm, wm, w_sem.at[4]))
    loads[4].start()

    start = hidden_ref[...].astype(f32)
    scale = lax.rsqrt(jnp.mean(start * start, axis=1, keepdims=True) + EPS)
    normed = (start * scale * gains_ref[0:1, :]).astype(bf16)
    last = (((1,), (1,)), ((), ()))
    in_all = lax.dot_general(normed, in_ref[...], last, preferred_element_type=f32)
    forget_all = lax.dot_general(normed, forget_ref[...], last, preferred_element_type=f32)
    forget_all = forget_all + bias_ref[...]
    forget_all = jnp.minimum(forget_all, 0.0) - jnp.log(1.0 + jnp.exp(-jnp.abs(forget_all)))
    column = lax.broadcasted_iota(jnp.int32, in_all.shape, 1)
    here = lax.broadcasted_iota(jnp.int32, (seqs, seqs), 0)
    there = lax.broadcasted_iota(jnp.int32, (seqs, seqs), 1)
    projected = []
    for i, weight in enumerate((wk, wq, wv)):
        loads[i].wait()
        product = jnp.dot(normed, weight[...], preferred_element_type=f32)
        projected.append(product.astype(bf16).astype(f32))
    keys, query, values = projected
    pieces = []
    for h in range(heads):
        span = slice(h * head, (h + 1) * head)
        pieces.extend((keys[:, span], query[:, span]))
    turned = jnp.concatenate(pieces, axis=0).T
    keeps = []
    adds = []
    bounds = []
    for h in range(heads):
        span = slice(h * head, (h + 1) * head)
        mine = column == tp * heads + h
        in_gate = jnp.sum(jnp.where(mine, in_all, 0.0), axis=1, keepdims=True)
        log_forget = jnp.sum(jnp.where(mine, forget_all, 0.0), axis=1, keepdims=True)
        before = jnp.sum(jnp.where(here == there, max_ref[h : h + 1, :], 0.0), axis=1, keepdims=True)
        carried = log_forget + before
        new_max = jnp.maximum(carried, in_gate)
        keep = jnp.exp(carried - new_max)
        write = jnp.exp(in_gate - new_max) * head ** (-0.5)
        new_max_ref[h : h + 1, :] = jnp.sum(
            jnp.where(here == there, new_max, 0.0), axis=0, keepdims=True
        )
        new_norm = keep * norm_ref[:, h, :] + write * keys[:, span]
        new_norm_ref[:, h, :] = new_norm
        denom = jnp.sum(query[:, span] * new_norm, axis=1, keepdims=True)
        bounds.append(jnp.maximum(jnp.abs(denom), jnp.exp(-new_max)))
        keeps.append(jnp.broadcast_to(keep, (seqs, head)))
        adds.append(write * values[:, span])
    stores = []
    for c in range(chunks):
        fetches[c].wait()
        for s in range(c * step, (c + 1) * step):
            for h in range(heads):
                at = 2 * h * seqs + s
                key_col = turned[:, at : at + 1]
                query_col = turned[:, at + seqs : at + seqs + 1]
                new = keeps[h][s : s + 1, :] * state[s, h] + key_col * adds[h][s : s + 1, :]
                state[s, h] = new
                numer[h, s : s + 1, :] = jnp.sum(query_col * new, axis=0, keepdims=True)
        rows = pl.ds(c * step, step)
        stores.append(pltpu.make_async_copy(state.at[rows], matrix_hbm.at[rows], out_sem.at[c]))
        stores[c].start()
    loads[3].wait()
    gate = jnp.dot(normed, wo[...], preferred_element_type=f32).astype(bf16).astype(f32)
    mixed = []
    for h in range(heads):
        span = slice(h * head, (h + 1) * head)
        mixed.append((jax.nn.sigmoid(gate[:, span]) * (numer[h] / bounds[h])).astype(bf16))
    mixed = jnp.concatenate(mixed, axis=1)
    loads[4].wait()
    part = terms_ref.shape[2]
    for t in range(terms_ref.shape[0]):
        terms_ref[t] = jnp.dot(
            mixed, wm[:, t * part : (t + 1) * part], preferred_element_type=f32
        ).astype(bf16)
    for store in stores:
        store.wait()


def front(hidden, norm_gains, gate_weights, forget_bias, state_norm, state_max, weights, state_matrix):
    tp_count = lax.axis_size("tp")
    seqs, width = hidden.shape
    heads, head = state_matrix.shape[1], state_matrix.shape[2]
    f32, bf16 = jnp.float32, jnp.bfloat16
    chunks = 4
    vmem = pl.BlockSpec(memory_space=pltpu.VMEM)
    hbm = pl.BlockSpec(memory_space=pl.ANY)
    terms, matrix, norm, top = pl.pallas_call(
        front_kernel,
        out_shape=(
            jax.ShapeDtypeStruct((tp_count, seqs, width // tp_count), bf16),
            jax.ShapeDtypeStruct(state_matrix.shape, f32),
            jax.ShapeDtypeStruct(state_norm.shape, f32),
            jax.ShapeDtypeStruct((heads, seqs), f32),
        ),
        in_specs=[vmem] * 7 + [hbm] * 6,
        out_specs=(vmem, hbm, vmem, vmem),
        scratch_shapes=[pltpu.VMEM(weight.shape, bf16) for weight in weights]
        + [
            pltpu.VMEM(state_matrix.shape, f32),
            pltpu.VMEM((heads, seqs, head), f32),
            pltpu.SemaphoreType.DMA((5,)),
            pltpu.SemaphoreType.DMA((chunks,)),
            pltpu.SemaphoreType.DMA((chunks,)),
        ],
        compiler_params=pltpu.CompilerParams(vmem_limit_bytes=67043328),
        name="front",
    )(
        hidden,
        norm_gains,
        gate_weights[0].T,
        gate_weights[1].T,
        forget_bias.reshape(1, -1),
        state_norm,
        state_max.T,
        *weights,
        state_matrix,
    )
    return terms, matrix, norm, top.T


MESH = pl.DeviceIdType.MESH


def tail_kernel(
    tp_count,
    ep_count,
    capacity,
    chunks,
    terms_hbm,
    hidden_hbm,
    gains_hbm,
    mix_hbm,
    routes_hbm,
    scores_hbm,
    eg_hbm,
    eu_hbm,
    ed_hbm,
    dg_hbm,
    du_hbm,
    dd_hbm,
    out_ref,
    terms,
    start_in,
    gains,
    mix,
    routes,
    scores,
    eg,
    eu,
    ed,
    dg,
    du,
    dd,
    br_recv,
    st_send,
    st_recv,
    fs_send,
    fs_recv,
    info_send,
    info_recv,
    mg_send,
    mg_recv,
    rows_in,
    xin,
    pre_send,
    pre_one,
    pre_mid,
    pre_two,
    hid,
    dense_out,
    eo_send,
    eo_one,
    eo_mid,
    eo_two,
    c_send,
    c_recv,
    s_sem,
    w_sem,
    tp_send,
    tp_recv,
    ep_send,
    ep_recv,
):
    tp = lax.axis_index("tp")
    ep = lax.axis_index("ep")
    seqs, part = start_in.shape
    width = part * tp_count
    per = ep_count // chunks
    chunk_rows = per * seqs
    chunk_slots = per * capacity
    quarter = chunk_rows // tp_count
    halves = 2
    half_chunks = chunks // halves
    half_slots = half_chunks * chunk_slots
    half_rows = half_chunks * chunk_rows
    first = pl.multiple_of(tp * part, part)
    f32, bf16 = jnp.float32, jnp.bfloat16

    own = pl.ds(first, part)
    smalls = []
    for i, (src, dst) in enumerate(
        (
            (terms_hbm, terms),
            (hidden_hbm.at[:, own], start_in),
            (gains_hbm.at[:, own], gains),
            (mix_hbm.at[:, own], mix),
            (routes_hbm, routes),
            (scores_hbm, scores),
        )
    ):
        load = pltpu.make_async_copy(src, dst, s_sem.at[i])
        load.start()
        smalls.append(load)

    barrier = pltpu.get_barrier_semaphore()
    for d in range(1, tp_count):
        pl.semaphore_signal(
            barrier, inc=1, device_id={"tp": lax.rem(tp + d, tp_count)}, device_id_type=MESH
        )
    for d in range(1, ep_count):
        pl.semaphore_signal(
            barrier, inc=1, device_id={"ep": lax.rem(ep + d, ep_count)}, device_id_type=MESH
        )

    loads = []
    for i, (src, dst) in enumerate(
        ((dg_hbm, dg), (du_hbm, du), (eg_hbm.at[0], eg), (eu_hbm.at[0], eu), (ed_hbm.at[0], ed), (dd_hbm, dd))
    ):
        load = pltpu.make_async_copy(src, dst, w_sem.at[i])
        load.start()
        loads.append(load)

    groups = tp_count // 2
    parity = lax.rem(tp, 2)
    group = tp // 2
    pair = tp + 1 - 2 * parity
    started = []
    tp_next = [0]
    ep_next = [0]

    def tp_copy(src, dst, peer):
        at = tp_next[0]
        tp_next[0] += 1
        copy = pltpu.make_async_remote_copy(
            src_ref=src,
            dst_ref=dst,
            send_sem=tp_send.at[at],
            recv_sem=tp_recv.at[at],
            device_id={"tp": peer},
            device_id_type=MESH,
        )
        copy.start()
        started.append(copy)
        return copy

    gray = [k ^ (k >> 1) for k in range(chunks)]
    order = [gray[k] * per + i for k in range(chunks) for i in range(per)]

    def partner(p):
        other = ep
        bit = 1
        while bit < ep_count:
            if order[p] & bit:
                other = other + bit * (1 - 2 * lax.rem(ep // bit, 2))
            bit *= 2
        return other

    def ep_copy(src, dst, p):
        at = ep_next[0]
        ep_next[0] += 1
        copy = pltpu.make_async_remote_copy(
            src_ref=src,
            dst_ref=dst,
            send_sem=ep_send.at[at],
            recv_sem=ep_recv.at[at],
            device_id={"ep": partner(p)},
            device_id_type=MESH,
        )
        copy.start()
        started.append(copy)
        return copy

    def tp_all(src_of, dst):
        made = []
        for d in range(1, tp_count):
            peer = lax.rem(tp + d, tp_count)
            made.append(tp_copy(src_of(peer), dst, peer))
        return made

    def ahead(d):
        return lax.rem(group + d, groups) * 2 + parity

    def behind(d):
        return lax.rem(group + groups - d, groups) * 2 + parity

    def gather_start(at):
        made = [tp_copy(at(tp), at(tp), ahead(d)) for d in range(1, groups)]
        made.append(tp_copy(at(tp), at(tp), pair))
        return made

    def gather_relay(at, made):
        for d in range(1, groups):
            made[d - 1].wait_recv()
            made.append(tp_copy(at(behind(d)), at(behind(d)), pair))

    def scatter_pair(at, one):
        return [tp_copy(at(j * 2 + 1 - parity), one(j), pair) for j in range(groups)]

    def scatter_cross(at, one, mid, two, made):
        arrive(made)
        for d in range(1, groups):
            j = lax.rem(group + d, groups)
            mid(j)[...] = (at(ahead(d))[...].astype(f32) + one(j)[...].astype(f32)).astype(bf16)
            made.append(tp_copy(mid(j), two(group), ahead(d)))

    def scatter_sum(at, one, two, made):
        total = at(tp)[...].astype(f32) + one(group)[...].astype(f32)
        for d in range(1, groups):
            made[groups + d - 1].wait_recv()
            total = total + two(lax.rem(group + groups - d, groups))[...].astype(f32)
        return total

    def arrive(copies):
        for copy in copies:
            copy.wait_recv()

    def from_tp(d):
        return lax.rem(tp + tp_count - d, tp_count)

    def columns(peer):
        return pl.ds(pl.multiple_of(peer * part, part), part)

    for ref in (st_send, fs_send, mg_send, info_send):
        ref[...] = jnp.zeros(ref.shape, f32)
    here = lax.broadcasted_iota(jnp.int32, (seqs, seqs), 0)
    there = lax.broadcasted_iota(jnp.int32, (seqs, seqs), 1)
    diagonal = here == there

    def to_row(column):
        return jnp.sum(jnp.where(diagonal, column, 0.0), axis=0, keepdims=True)

    def to_column(row):
        return jnp.sum(jnp.where(diagonal, row, 0.0), axis=1, keepdims=True)

    for load in smalls:
        load.wait()
    pl.semaphore_wait(barrier, tp_count - 1 + ep_count - 1)
    branch_copies = tp_all(lambda peer: terms.at[peer], br_recv.at[tp])

    top = routes.shape[0]
    experts = info_send.shape[1]
    name = lax.broadcasted_iota(jnp.int32, (experts, seqs), 0)
    hits = [routes[k : k + 1, :] == name for k in range(top)]
    named = hits[0]
    for k in range(1, top):
        named = jnp.logical_or(named, hits[k])
    named = jnp.where(named, 1.0, 0.0)
    before = jnp.where(here < there, 1.0, 0.0).astype(bf16)
    rank = jnp.dot(named.astype(bf16), before, preferred_element_type=f32) + 1.0
    score_sum = scores[0:1, :]
    for k in range(1, top):
        score_sum = score_sum + scores[k : k + 1, :]
    share = jnp.zeros((experts, seqs), f32)
    for k in range(top):
        share = share + jnp.where(hits[k], scores[k : k + 1, :] / score_sum, 0.0)
    info_send[0, :, 0:seqs] = named * rank
    info_send[1, :, 0:seqs] = share
    info_copies = [ep_copy(info_send, info_recv.at[p], p) for p in range(1, ep_count)]

    start_part = start_in[...].astype(f32)
    gain_one = gains[1:2, :]
    gain_two = gains[2:3, :]
    gain_three = gains[3:4, :]
    mix_weight = gain_two * mix[...]
    start_sq = jnp.sum(start_part * start_part, axis=1, keepdims=True)
    start_dot = jnp.sum(start_part * mix_weight, axis=1, keepdims=True)
    branch = terms[tp].astype(f32)
    arrive(branch_copies)
    for d in range(1, tp_count):
        branch = branch + br_recv[from_tp(d)].astype(f32)
    branch = branch.astype(bf16).astype(f32)
    lifted = gain_one * branch
    sums = (
        jnp.sum(branch * branch, axis=1, keepdims=True),
        start_sq,
        jnp.sum(start_part * lifted, axis=1, keepdims=True),
        jnp.sum(lifted * lifted, axis=1, keepdims=True),
        start_dot,
        jnp.sum(lifted * mix_weight, axis=1, keepdims=True),
    )
    for i, value in enumerate(sums):
        st_send[i : i + 1, 0:seqs] = to_row(value)
    stat_copies = tp_all(lambda peer: st_send, st_recv.at[tp])
    packed = st_send[...]
    arrive(stat_copies)
    for d in range(1, tp_count):
        packed = packed + st_recv[from_tp(d)]
    branch_sq, start_sq, cross_sum, lifted_sq, start_dot, lifted_dot = (
        packed[i : i + 1, 0:seqs] for i in range(6)
    )
    branch_scale = lax.rsqrt(branch_sq / width + EPS)
    resid_sq = start_sq + 2.0 * branch_scale * cross_sum + branch_scale * branch_scale * lifted_sq
    gate_dot = start_dot + branch_scale * lifted_dot
    scale_two = lax.rsqrt(resid_sq / width + EPS)
    mg_send[0:1, 0:seqs] = jax.nn.sigmoid(scale_two * gate_dot)
    residual_f = start_part + lifted * to_column(branch_scale)
    residual = residual_f.astype(bf16).astype(f32)
    rows_in[0] = (residual_f * to_column(scale_two) * gain_two).astype(bf16)
    row_copies = [ep_copy(rows_in.at[0], rows_in.at[p], p) for p in range(1, ep_count)]
    mg_copies = [ep_copy(mg_send, mg_recv.at[p], p) for p in range(1, ep_count)]

    mine = lax.broadcasted_iota(jnp.int32, (experts, seqs), 0) == ep
    wanted = (lax.broadcasted_iota(jnp.int32, (capacity, seqs), 0) + 1).astype(f32)
    placings = []
    shares = []

    def place(p):
        if p == 0:
            codes, portion = info_send[0], info_send[1]
        else:
            info_copies[p - 1].wait_recv()
            codes, portion = info_recv[p, 0], info_recv[p, 1]
        code = jnp.sum(jnp.where(mine, codes[:, 0:seqs], 0.0), axis=0, keepdims=True)
        placings.append(jnp.where(code == wanted, 1.0, 0.0).astype(bf16))
        shares.append(jnp.sum(jnp.where(mine, portion[:, 0:seqs], 0.0), axis=0, keepdims=True))

    def slots_of(p):
        return pl.ds(p * capacity, capacity)

    def xin_at(k):
        return lambda i: xin.at[i, pl.ds(k * chunk_slots, chunk_slots)]

    def pre_at(k):
        return lambda i: pre_send.at[k, i]

    def of(ref, k):
        return lambda j: ref.at[k, j]

    def hid_at(k):
        return lambda i: hid.at[k, i]

    def half_of(ref, h):
        return lambda i: ref.at[i, pl.ds(h * half_slots, half_slots)]

    last = (((1,), (1,)), ((), ()))
    xin_copies = []
    pre_copies = []
    hid_copies = []

    def chunk_in(k):
        for p in range(k * per, (k + 1) * per):
            place(p)
            if p > 0:
                row_copies[p - 1].wait_recv()
            xin[tp, slots_of(p)] = jnp.dot(
                placings[p], rows_in[p], preferred_element_type=f32
            ).astype(bf16)
        xin_copies.append(gather_start(xin_at(k)))
        if k == 0:
            loads[0].wait()
            loads[1].wait()
        rows = rows_in[k * per : (k + 1) * per].reshape(chunk_rows, part)
        for i, weight in enumerate((dg, du)):
            made = lax.dot_general(rows, weight[...], last, preferred_element_type=f32).astype(bf16)
            for t in range(tp_count):
                pre_send[k, t, i] = made[t * quarter : (t + 1) * quarter]
        pre_copies.append(scatter_pair(pre_at(k), of(pre_one, k)))

    def pre_cross(k):
        scatter_cross(pre_at(k), of(pre_one, k), of(pre_mid, k), of(pre_two, k), pre_copies[k])

    def pre_done(k):
        pre = scatter_sum(pre_at(k), of(pre_one, k), of(pre_two, k), pre_copies[k])
        hid[k, tp] = (jax.nn.silu(pre[0]) * pre[1]).astype(bf16)
        hid_copies.append(gather_start(hid_at(k)))

    def xin_relay(k):
        gather_relay(xin_at(k), xin_copies[k])

    def hid_relay(k):
        gather_relay(hid_at(k), hid_copies[k])

    sums_of = [None, None]

    def expert_in(source):
        for i, weight in enumerate((eg, eu)):
            made = jnp.dot(xin[source], weight[columns(source), :], preferred_element_type=f32)
            sums_of[i] = made if sums_of[i] is None else sums_of[i] + made

    for k in range(chunks):
        chunk_in(k)
        if k >= 1:
            pre_cross(k - 1)
        if k >= 2:
            xin_relay(k - 2)
    if chunks >= 2:
        xin_relay(chunks - 2)
    loads[2].wait()
    loads[3].wait()
    expert_in(tp)
    pre_cross(chunks - 1)
    pre_done(0)
    for k in range(chunks):
        xin_copies[k][groups - 1].wait_recv()
    expert_in(pair)
    xin_relay(chunks - 1)
    pre_done(1)
    for d in range(1, groups):
        expert_in(behind(d))
    pre_done(2)
    for d in range(1, groups):
        for k in range(chunks):
            xin_copies[k][groups - 1 + d].wait_recv()
        expert_in(behind(d) + 1 - 2 * parity)
    hidden_units = (jax.nn.silu(sums_of[0]) * sums_of[1]).astype(bf16)

    loads[4].wait()
    eo_copies = [None] * halves
    turn = list(range(halves))[::-1]

    def expert_down(h, t):
        eo_send[t, h * half_slots : (h + 1) * half_slots] = jnp.dot(
            hidden_units[h * half_slots : (h + 1) * half_slots],
            ed[:, columns(t)],
            preferred_element_type=f32,
        ).astype(bf16)

    for h in turn:
        for j in range(groups):
            expert_down(h, j * 2 + 1 - parity)
        eo_copies[h] = scatter_pair(half_of(eo_send, h), half_of(eo_one, h))
    for k in range(3, chunks):
        pre_done(k)
    for k in range(chunks - 1):
        hid_relay(k)
    for h in turn:
        for j in range(groups):
            expert_down(h, j * 2 + parity)
        scatter_cross(
            half_of(eo_send, h), half_of(eo_one, h), half_of(eo_mid, h), half_of(eo_two, h), eo_copies[h]
        )
    hid_relay(chunks - 1)
    loads[5].wait()
    c_copies = {}
    mixed = None
    for h in turn:
        for k in range(h * half_chunks, (h + 1) * half_chunks):
            arrive(hid_copies[k][groups - 1 :])
        units = hid.shape[3]
        dense_out[h * half_rows : (h + 1) * half_rows] = jnp.dot(
            hid[h * half_chunks : (h + 1) * half_chunks].reshape(half_rows, units),
            dd[...],
            preferred_element_type=f32,
        )
    first_dims = (((0,), (0,)), ((), ()))
    for h in turn:
        total = scatter_sum(half_of(eo_send, h), half_of(eo_one, h), half_of(eo_two, h), eo_copies[h])
        total = total.astype(bf16)
        for q in list(range(half_chunks * per))[::-1]:
            p = h * half_chunks * per + q
            picked = lax.dot_general(
                placings[p],
                total[q * capacity : (q + 1) * capacity],
                first_dims,
                preferred_element_type=f32,
            )
            if p == 0:
                gate = mg_send[0:1, 0:seqs]
            else:
                mg_copies[p - 1].wait_recv()
                gate = mg_recv[p, 0:1, 0:seqs]
            combined = (
                to_column(gate) * dense_out[p * seqs : (p + 1) * seqs] + to_column(shares[p]) * picked
            )
            if p == 0:
                mixed = combined
            else:
                c_send[p] = combined.astype(bf16)
                c_copies[p] = ep_copy(c_send.at[p], c_recv.at[p], p)
    ffn = mixed
    for p in range(1, ep_count):
        c_copies[p].wait_recv()
        ffn = ffn + c_recv[p].astype(f32)
    fs_send[0:1, 0:seqs] = to_row(jnp.sum(ffn * ffn, axis=1, keepdims=True))
    final_copies = tp_all(lambda peer: fs_send, fs_recv.at[tp])
    scaled = gain_three * ffn
    squares = fs_send[...]
    arrive(final_copies)
    for d in range(1, tp_count):
        squares = squares + fs_recv[from_tp(d)]
    scale = to_column(lax.rsqrt(squares[0:1, 0:seqs] / width + EPS))
    out_ref[...] = (residual + scaled * scale).astype(bf16)
    for copy in started:
        copy.wait_send()


def tail(
    terms, hidden, norm_gains, dense_mix, routes, route_scores, weights
):
    tp_count = lax.axis_size("tp")
    ep_count = lax.axis_size("ep")
    seqs, width = hidden.shape
    part = width // tp_count
    expert_gate, expert_up, expert_down, dense_gate, dense_up, dense_down = weights
    units = expert_gate.shape[2]
    dense_gate, dense_up = dense_gate.T, dense_up.T
    dense_units = dense_gate.shape[0]
    top = routes.shape[1]
    experts = ep_count * expert_gate.shape[0]
    limit = 2 * seqs * top // ep_count
    capacity = -(-limit // 16) * 16
    chunks = 4
    rows_all = ep_count * seqs
    quarter = rows_all // chunks // tp_count
    groups = tp_count // 2
    lanes = -(-seqs // 128) * 128
    f32, bf16 = jnp.float32, jnp.bfloat16
    vmem = pl.BlockSpec(memory_space=pltpu.VMEM)
    hbm = pl.BlockSpec(memory_space=pl.ANY)
    slots = ep_count * capacity
    tp_copies = 3 * (tp_count - 1) + (3 * chunks + 2) * (2 * groups - 1)
    ep_copies = 4 * (ep_count - 1)
    piece = pltpu.VMEM((chunks, groups, 2, quarter, dense_units), bf16)
    return pl.pallas_call(
        functools.partial(tail_kernel, tp_count, ep_count, capacity, chunks),
        out_shape=jax.ShapeDtypeStruct((seqs, part), bf16),
        in_specs=[hbm] * 12,
        out_specs=vmem,
        scratch_shapes=[
            pltpu.VMEM((tp_count, seqs, part), bf16),
            pltpu.VMEM((seqs, part), bf16),
            pltpu.VMEM((norm_gains.shape[0], part), f32),
            pltpu.VMEM((1, part), f32),
            pltpu.VMEM((top, seqs), jnp.int32),
            pltpu.VMEM((top, seqs), f32),
            pltpu.VMEM((width, units), bf16),
            pltpu.VMEM((width, units), bf16),
            pltpu.VMEM((units, width), bf16),
            pltpu.VMEM(dense_gate.shape, bf16),
            pltpu.VMEM(dense_up.shape, bf16),
            pltpu.VMEM(dense_down.shape, bf16),
            pltpu.VMEM((tp_count, seqs, part), bf16),
            pltpu.VMEM((8, lanes), f32),
            pltpu.VMEM((tp_count, 8, lanes), f32),
            pltpu.VMEM((1, lanes), f32),
            pltpu.VMEM((tp_count, 1, lanes), f32),
            pltpu.VMEM((2, experts, lanes), f32),
            pltpu.VMEM((ep_count, 2, experts, lanes), f32),
            pltpu.VMEM((1, lanes), f32),
            pltpu.VMEM((ep_count, 1, lanes), f32),
            pltpu.VMEM((ep_count, seqs, part), bf16),
            pltpu.VMEM((tp_count, slots, part), bf16),
            pltpu.VMEM((chunks, tp_count, 2, quarter, dense_units), bf16),
            piece,
            piece,
            piece,
            pltpu.VMEM((chunks, tp_count, quarter, dense_units), bf16),
            pltpu.VMEM((rows_all, part), f32),
            pltpu.VMEM((tp_count, slots, part), bf16),
            pltpu.VMEM((groups, slots, part), bf16),
            pltpu.VMEM((groups, slots, part), bf16),
            pltpu.VMEM((groups, slots, part), bf16),
            pltpu.VMEM((ep_count, seqs, part), bf16),
            pltpu.VMEM((ep_count, seqs, part), bf16),
            pltpu.SemaphoreType.DMA((6,)),
            pltpu.SemaphoreType.DMA((6,)),
            pltpu.SemaphoreType.DMA((tp_copies,)),
            pltpu.SemaphoreType.DMA((tp_copies,)),
            pltpu.SemaphoreType.DMA((ep_copies,)),
            pltpu.SemaphoreType.DMA((ep_copies,)),
        ],
        compiler_params=pltpu.CompilerParams(
            collective_id=0, has_side_effects=True, vmem_limit_bytes=67043328
        ),
        name="tail",
    )(
        terms,
        hidden,
        norm_gains,
        dense_mix.reshape(1, width),
        routes.T,
        route_scores.T,
        expert_gate,
        expert_up,
        expert_down,
        dense_gate,
        dense_up,
        dense_down,
    )


def local(
    hidden,
    norm_gains,
    w_query,
    w_key,
    w_value,
    w_outgate,
    w_input_gate,
    w_forget_gate,
    forget_bias,
    w_mix_out,
    state_matrix,
    state_norm,
    state_max,
    routes,
    route_scores,
    expert_gate,
    expert_up,
    expert_down,
    dense_gate,
    dense_up,
    dense_down,
    dense_mix,
):
    terms, new_matrix, new_norm, new_max = front(
        hidden,
        norm_gains,
        (w_input_gate, w_forget_gate),
        forget_bias,
        state_norm,
        state_max,
        (w_query, w_key, w_value, w_outgate, w_mix_out),
        state_matrix,
    )
    new_hidden = tail(
        terms,
        hidden,
        norm_gains,
        dense_mix,
        routes,
        route_scores,
        (expert_gate, expert_up, expert_down, dense_gate, dense_up, dense_down),
    )
    return (new_hidden, new_matrix, new_norm, new_max)


def solution(mesh):
    placed = (
        P("ep", None),
        P(),
        P(None, "tp"),
        P(None, "tp"),
        P(None, "tp"),
        P(None, "tp"),
        P(),
        P(),
        P(),
        P("tp", None),
        P("ep", "tp", None, None),
        P("ep", "tp", None),
        P("ep", "tp"),
        P("ep", None),
        P("ep", None),
        P("ep", None, "tp"),
        P("ep", None, "tp"),
        P("ep", "tp", None),
        P("tp", "ep"),
        P("tp", "ep"),
        P("ep", "tp"),
        P(),
    )
    return jax.shard_map(
        local,
        mesh=mesh,
        in_specs=placed,
        out_specs=(P("ep", "tp"), P("ep", "tp", None, None), P("ep", "tp", None), P("ep", "tp")),
        check_vma=False,
    )
```

```python
import functools

import jax
import jax.numpy as jnp
from jax import lax
from jax.experimental import pallas as pl
from jax.experimental.pallas import tpu as pltpu
from jax.sharding import PartitionSpec as P

EPS = 1e-06


def front_kernel(
    hidden_hbm,
    gains_hbm,
    in_hbm,
    forget_hbm,
    bias_hbm,
    norm_hbm,
    max_hbm,
    wq_hbm,
    wk_hbm,
    wv_hbm,
    wo_hbm,
    wm_hbm,
    state_hbm,
    terms_hbm,
    matrix_hbm,
    new_norm_hbm,
    new_max_ref,
    wq,
    wk,
    wv,
    wo,
    wm,
    hidden,
    gains,
    in_weight,
    forget_weight,
    bias,
    norm,
    top,
    state,
    numer,
    terms,
    new_norms,
    s_sem,
    w_sem,
    in_sem,
    out_sem,
    end_sem,
):
    tp = lax.axis_index("tp")
    f32, bf16 = jnp.float32, jnp.bfloat16
    seqs = hidden.shape[0]
    heads, head = state.shape[1], state.shape[2]
    chunks = in_sem.shape[0]
    step = seqs // chunks
    smalls = []
    for i, (src, dst) in enumerate(
        (
            (hidden_hbm, hidden),
            (gains_hbm, gains),
            (in_hbm, in_weight),
            (forget_hbm, forget_weight),
            (bias_hbm, bias),
            (max_hbm, top),
            (norm_hbm, norm),
        )
    ):
        smalls.append(pltpu.make_async_copy(src, dst, s_sem.at[i]))
    for small in smalls[:4]:
        small.start()
    loads = []
    for i, (src, dst) in enumerate(((wk_hbm, wk), (wq_hbm, wq), (wv_hbm, wv), (wo_hbm, wo), (wm_hbm, wm))):
        loads.append(pltpu.make_async_copy(src, dst, w_sem.at[i]))
    fetches = []
    for c in range(chunks):
        rows = pl.ds(c * step, step)
        fetches.append(pltpu.make_async_copy(state_hbm.at[rows], state.at[rows], in_sem.at[c]))
    for load in loads[:3]:
        load.start()
    for small in smalls[4:]:
        small.start()
    for small in smalls[:4]:
        small.wait()
    for fetch in fetches:
        fetch.start()
    for load in loads[3:]:
        load.start()

    start = hidden[...].astype(f32)
    scale = lax.rsqrt(jnp.mean(start * start, axis=1, keepdims=True) + EPS)
    normed = (start * scale * gains[0:1, :]).astype(bf16)
    last = (((1,), (1,)), ((), ()))
    in_all = lax.dot_general(normed, in_weight[...], last, preferred_element_type=f32)
    forget_all = lax.dot_general(normed, forget_weight[...], last, preferred_element_type=f32)
    column = lax.broadcasted_iota(jnp.int32, in_all.shape, 1)
    here = lax.broadcasted_iota(jnp.int32, (seqs, seqs), 0)
    there = lax.broadcasted_iota(jnp.int32, (seqs, seqs), 1)
    projected = []
    for i, weight in enumerate((wk, wq, wv)):
        loads[i].wait()
        product = jnp.dot(normed, weight[...], preferred_element_type=f32)
        projected.append(product.astype(bf16).astype(f32))
    keys, query, values = projected
    for small in smalls[4:]:
        small.wait()
    forget_all = forget_all + bias[...]
    forget_all = jnp.minimum(forget_all, 0.0) - jnp.log(1.0 + jnp.exp(-jnp.abs(forget_all)))
    keeps = []
    bounds = []
    outers = []
    turns = []
    for h in range(heads):
        span = slice(h * head, (h + 1) * head)
        mine = column == tp * heads + h
        in_gate = jnp.sum(jnp.where(mine, in_all, 0.0), axis=1, keepdims=True)
        log_forget = jnp.sum(jnp.where(mine, forget_all, 0.0), axis=1, keepdims=True)
        before = jnp.sum(jnp.where(here == there, top[h : h + 1, :], 0.0), axis=1, keepdims=True)
        carried = log_forget + before
        new_max = jnp.maximum(carried, in_gate)
        keep = jnp.exp(carried - new_max)
        write = jnp.exp(in_gate - new_max) * head ** (-0.5)
        new_max_ref[h : h + 1, :] = jnp.sum(
            jnp.where(here == there, new_max, 0.0), axis=0, keepdims=True
        )
        new_norm = keep * norm[:, h, :] + write * keys[:, span]
        new_norms[:, h, :] = new_norm
        denom = jnp.sum(query[:, span] * new_norm, axis=1, keepdims=True)
        bounds.append(jnp.maximum(jnp.abs(denom), jnp.exp(-new_max)))
        keeps.append(jnp.broadcast_to(keep, (seqs, head)))
        added = write * values[:, span]
        high = added.astype(bf16).astype(f32)
        middle = (added - high).astype(bf16).astype(f32)
        low = (added - high - middle).astype(bf16).astype(f32)
        outers.append(jnp.concatenate([high, middle, low, jnp.zeros_like(low)], axis=0))
        turned = jnp.concatenate([keys[:, span]] * 3 + [query[:, span]], axis=0).T
        turns.append((turned, turned.astype(bf16)))
    norm_store = pltpu.make_async_copy(new_norms, new_norm_hbm, end_sem.at[0])
    norm_store.start()
    from_seq = lax.rem(lax.broadcasted_iota(jnp.int32, outers[0].shape, 0), seqs)
    stores = []
    for c in range(chunks):
        fetches[c].wait()
        for s in range(c * step, (c + 1) * step, 2):
            for h in range(heads):
                turned, turned_half = turns[h]
                picked = [jnp.where(from_seq == s + i, outers[h], 0.0).astype(bf16) for i in range(2)]
                written = jnp.dot(
                    turned_half, jnp.concatenate(picked, axis=1), preferred_element_type=f32
                )
                for i in range(2):
                    at = 3 * seqs + s + i
                    query_col = turned[:, at : at + 1]
                    new = (
                        keeps[h][s + i : s + i + 1, :] * state[s + i, h]
                        + written[:, i * head : (i + 1) * head]
                    )
                    state[s + i, h] = new
                    numer[h, s + i : s + i + 1, :] = jnp.sum(query_col * new, axis=0, keepdims=True)
        rows = pl.ds(c * step, step)
        stores.append(pltpu.make_async_copy(state.at[rows], matrix_hbm.at[rows], out_sem.at[c]))
        stores[c].start()
    loads[3].wait()
    gate = jnp.dot(normed, wo[...], preferred_element_type=f32).astype(bf16).astype(f32)
    mixed = []
    for h in range(heads):
        span = slice(h * head, (h + 1) * head)
        mixed.append((jax.nn.sigmoid(gate[:, span]) * (numer[h] / bounds[h])).astype(bf16))
    mixed = jnp.concatenate(mixed, axis=1)
    loads[4].wait()
    part = terms.shape[2]
    for t in range(terms.shape[0]):
        terms[t] = jnp.dot(
            mixed, wm[:, t * part : (t + 1) * part], preferred_element_type=f32
        ).astype(bf16)
    terms_store = pltpu.make_async_copy(terms, terms_hbm, end_sem.at[1])
    terms_store.start()
    for store in stores + [norm_store, terms_store]:
        store.wait()


def front(hidden, norm_gains, gate_weights, forget_bias, state_norm, state_max, weights, state_matrix):
    tp_count = lax.axis_size("tp")
    seqs, width = hidden.shape
    heads, head = state_matrix.shape[1], state_matrix.shape[2]
    f32, bf16 = jnp.float32, jnp.bfloat16
    chunks = 4
    vmem = pl.BlockSpec(memory_space=pltpu.VMEM)
    hbm = pl.BlockSpec(memory_space=pl.ANY)
    smalls = (
        hidden,
        norm_gains,
        gate_weights[0].T,
        gate_weights[1].T,
        forget_bias.reshape(1, -1),
        state_norm,
        state_max.T,
    )
    terms, matrix, norm, top = pl.pallas_call(
        front_kernel,
        out_shape=(
            jax.ShapeDtypeStruct((tp_count, seqs, width // tp_count), bf16),
            jax.ShapeDtypeStruct(state_matrix.shape, f32),
            jax.ShapeDtypeStruct(state_norm.shape, f32),
            jax.ShapeDtypeStruct((heads, seqs), f32),
        ),
        in_specs=[hbm] * 13,
        out_specs=(hbm, hbm, hbm, vmem),
        scratch_shapes=[pltpu.VMEM(weight.shape, bf16) for weight in weights]
        + [pltpu.VMEM(small.shape, small.dtype) for small in smalls]
        + [
            pltpu.VMEM(state_matrix.shape, f32),
            pltpu.VMEM((heads, seqs, head), f32),
            pltpu.VMEM((tp_count, seqs, width // tp_count), bf16),
            pltpu.VMEM(state_norm.shape, f32),
            pltpu.SemaphoreType.DMA((7,)),
            pltpu.SemaphoreType.DMA((5,)),
            pltpu.SemaphoreType.DMA((chunks,)),
            pltpu.SemaphoreType.DMA((chunks,)),
            pltpu.SemaphoreType.DMA((2,)),
        ],
        compiler_params=pltpu.CompilerParams(vmem_limit_bytes=67043328),
        name="front",
    )(*smalls, *weights, state_matrix)
    return terms, matrix, norm, top.T


MESH = pl.DeviceIdType.MESH


def tail_kernel(
    tp_count,
    ep_count,
    capacity,
    chunks,
    terms_hbm,
    hidden_hbm,
    gains_hbm,
    mix_hbm,
    routes_hbm,
    scores_hbm,
    eg_hbm,
    eu_hbm,
    ed_hbm,
    dg_hbm,
    du_hbm,
    dd_hbm,
    out_ref,
    terms,
    start_in,
    gains,
    mix,
    routes,
    scores,
    eg,
    eu,
    ed,
    dg,
    du,
    dd,
    dgt,
    dut,
    br_recv,
    st_send,
    st_recv,
    fs_send,
    fs_recv,
    info_send,
    info_recv,
    mg_send,
    mg_recv,
    rows_in,
    xin,
    pre_send,
    pre_one,
    pre_mid,
    pre_two,
    hid,
    dense_out,
    eo_send,
    eo_one,
    eo_mid,
    eo_two,
    c_send,
    c_recv,
    s_sem,
    w_sem,
    join_sem,
    go_sem,
    tp_send,
    tp_recv,
    ep_send,
    ep_recv,
):
    tp = lax.axis_index("tp")
    ep = lax.axis_index("ep")
    seqs, part = start_in.shape
    width = part * tp_count
    per = ep_count // chunks
    chunk_rows = per * seqs
    chunk_slots = per * capacity
    quarter = chunk_rows // tp_count
    first = pl.multiple_of(tp * part, part)
    f32, bf16 = jnp.float32, jnp.bfloat16

    own = pl.ds(first, part)
    smalls = []
    for i, (src, dst) in enumerate(
        (
            (terms_hbm, terms),
            (hidden_hbm.at[:, own], start_in),
            (gains_hbm.at[:, own], gains),
            (mix_hbm.at[:, own], mix),
            (routes_hbm, routes),
            (scores_hbm, scores),
        )
    ):
        load = pltpu.make_async_copy(src, dst, s_sem.at[i])
        load.start()
        smalls.append(load)

    gray = [k ^ (k >> 1) for k in range(chunks)]
    order = [gray[k] * per + i for k in range(chunks) for i in range(per)]

    def partner(p):
        other = ep
        bit = 1
        while bit < ep_count:
            if order[p] & bit:
                other = other + bit * (1 - 2 * lax.rem(ep // bit, 2))
            bit *= 2
        return other

    barrier = pltpu.get_barrier_semaphore()
    for d in range(1, tp_count):
        peer = lax.rem(tp + d, tp_count)

        @pl.when(peer != 0)
        def _(peer=peer):
            pl.semaphore_signal(barrier, inc=1, device_id={"tp": peer}, device_id_type=MESH)

    loads = []
    for i, (src, dst) in enumerate(
        ((dg_hbm, dg), (du_hbm, du), (eg_hbm.at[0], eg), (eu_hbm.at[0], eu), (ed_hbm.at[0], ed), (dd_hbm, dd))
    ):
        load = pltpu.make_async_copy(src, dst, w_sem.at[i])
        load.start()
        loads.append(load)

    groups = tp_count // 2
    parity = lax.rem(tp, 2)
    group = tp // 2
    pair = tp + 1 - 2 * parity
    started = []
    tp_next = [0]
    ep_next = [0]

    def tp_copy(src, dst, peer):
        at = tp_next[0]
        tp_next[0] += 1
        copy = pltpu.make_async_remote_copy(
            src_ref=src,
            dst_ref=dst,
            send_sem=tp_send.at[at],
            recv_sem=tp_recv.at[at],
            device_id={"tp": peer},
            device_id_type=MESH,
        )
        copy.start()
        started.append(copy)
        return copy

    def ep_copy(src, dst, p):
        at = ep_next[0]
        ep_next[0] += 1
        copy = pltpu.make_async_remote_copy(
            src_ref=src,
            dst_ref=dst,
            send_sem=ep_send.at[at],
            recv_sem=ep_recv.at[at],
            device_id={"ep": partner(p)},
            device_id_type=MESH,
        )
        copy.start()
        started.append(copy)
        return copy

    def tp_all(src_of, dst):
        made = []
        for d in range(1, tp_count):
            peer = lax.rem(tp + d, tp_count)
            made.append(tp_copy(src_of(peer), dst, peer))
        return made

    def ahead(d):
        return lax.rem(group + d, groups) * 2 + parity

    def behind(d):
        return lax.rem(group + groups - d, groups) * 2 + parity

    def gather_start(at):
        made = [tp_copy(at(tp), at(tp), ahead(d)) for d in range(1, groups)]
        made.append(tp_copy(at(tp), at(tp), pair))
        return made

    def gather_relay(at, made):
        for d in range(1, groups):
            made[d - 1].wait_recv()
            made.append(tp_copy(at(behind(d)), at(behind(d)), pair))

    def scatter_pair(at, one):
        return [tp_copy(at(j * 2 + 1 - parity), one(j), pair) for j in range(groups)]

    def scatter_cross(at, one, mid, two, made):
        arrive(made)
        for d in range(1, groups):
            j = lax.rem(group + d, groups)
            mid(j)[...] = (at(ahead(d))[...].astype(f32) + one(j)[...].astype(f32)).astype(bf16)
            made.append(tp_copy(mid(j), two(group), ahead(d)))

    def scatter_sum(at, one, two, made):
        total = at(tp)[...].astype(f32) + one(group)[...].astype(f32)
        for d in range(1, groups):
            made[groups + d - 1].wait_recv()
            total = total + two(lax.rem(group + groups - d, groups))[...].astype(f32)
        return total

    def arrive(copies):
        for copy in copies:
            copy.wait_recv()

    def from_tp(d):
        return lax.rem(tp + tp_count - d, tp_count)

    def columns(peer):
        return pl.ds(pl.multiple_of(peer * part, part), part)

    for ref in (fs_send, mg_send, info_send):
        ref[...] = jnp.zeros(ref.shape, f32)
    here = lax.broadcasted_iota(jnp.int32, (seqs, seqs), 0)
    there = lax.broadcasted_iota(jnp.int32, (seqs, seqs), 1)
    diagonal = here == there

    def to_row(column):
        return jnp.sum(jnp.where(diagonal, column, 0.0), axis=0, keepdims=True)

    def to_column(row):
        return jnp.sum(jnp.where(diagonal, row, 0.0), axis=1, keepdims=True)

    for load in smalls:
        load.wait()

    @pl.when(tp != 0)
    def _():
        pl.semaphore_wait(barrier, tp_count - 1)
        pl.semaphore_signal(join_sem, inc=1, device_id={"tp": 0}, device_id_type=MESH)

    @pl.when(tp == 0)
    def _():
        pl.semaphore_wait(join_sem, tp_count - 1)
        for p in range(1, ep_count):
            pl.semaphore_signal(barrier, inc=1, device_id={"ep": partner(p)}, device_id_type=MESH)

    branch_copies = tp_all(lambda peer: terms.at[peer], br_recv.at[tp])

    top = routes.shape[0]
    experts = info_send.shape[1]
    name = lax.broadcasted_iota(jnp.int32, (experts, seqs), 0)
    hits = [routes[k : k + 1, :] == name for k in range(top)]
    named = hits[0]
    for k in range(1, top):
        named = jnp.logical_or(named, hits[k])
    named = jnp.where(named, 1.0, 0.0)
    before = jnp.where(here < there, 1.0, 0.0).astype(bf16)
    rank = jnp.dot(named.astype(bf16), before, preferred_element_type=f32) + 1.0
    score_sum = scores[0:1, :]
    for k in range(1, top):
        score_sum = score_sum + scores[k : k + 1, :]
    share = jnp.zeros((experts, seqs), f32)
    for k in range(top):
        share = share + jnp.where(hits[k], scores[k : k + 1, :] / score_sum, 0.0)
    info_send[0, :, 0:seqs] = named * rank
    info_send[1, :, 0:seqs] = share

    start_part = start_in[...].astype(f32)
    gain_one = gains[1:2, :]
    gain_two = gains[2:3, :]
    gain_three = gains[3:4, :]
    mix_weight = gain_two * mix[...]
    start_sq = jnp.sum(start_part * start_part, axis=1, keepdims=True)
    start_dot = jnp.sum(start_part * mix_weight, axis=1, keepdims=True)
    branch = terms[tp].astype(f32)
    loads[0].wait()
    dgt[...] = dg[...].T
    arrive(branch_copies)
    for d in range(1, tp_count):
        branch = branch + br_recv[from_tp(d)].astype(f32)
    branch = branch.astype(bf16).astype(f32)
    lifted = gain_one * branch
    lanes = st_send.shape[1]
    lane = lax.broadcasted_iota(jnp.int32, (seqs, lanes), 1)
    place_of = lax.broadcasted_iota(jnp.int32, (seqs, lanes), 0)

    def pack(values):
        made = jnp.zeros((seqs, lanes), f32)
        for i, value in enumerate(values):
            made = jnp.where(lane == place_of + i * seqs, value, made)
        return jnp.sum(made, axis=0, keepdims=True)

    def unpack(row, i):
        return jnp.sum(jnp.where(lane == place_of + i * seqs, row, 0.0), axis=1, keepdims=True)

    packed = pack(
        (
            jnp.sum(branch * branch, axis=1, keepdims=True),
            start_sq,
            jnp.sum(start_part * lifted, axis=1, keepdims=True),
            jnp.sum(lifted * lifted, axis=1, keepdims=True),
            start_dot,
            jnp.sum(lifted * mix_weight, axis=1, keepdims=True),
        )
    )
    st_send[...] = packed
    stat_copies = tp_all(lambda peer: st_send, st_recv.at[tp])

    @pl.when(tp == 0)
    def _():
        pl.semaphore_wait(barrier, ep_count - 1)
        for t in range(1, tp_count):
            pl.semaphore_signal(go_sem, inc=1, device_id={"tp": t}, device_id_type=MESH)

    @pl.when(tp != 0)
    def _():
        pl.semaphore_wait(go_sem, 1)

    info_copies = [ep_copy(info_send, info_recv.at[p], p) for p in range(1, ep_count)]
    loads[1].wait()
    dut[...] = du[...].T
    arrive(stat_copies)
    for d in range(1, tp_count):
        packed = packed + st_recv[from_tp(d)]
    branch_sq, start_sq, cross_sum, lifted_sq, start_dot, lifted_dot = (
        unpack(packed, i) for i in range(6)
    )
    branch_scale = lax.rsqrt(branch_sq / width + EPS)
    resid_sq = start_sq + 2.0 * branch_scale * cross_sum + branch_scale * branch_scale * lifted_sq
    gate_dot = start_dot + branch_scale * lifted_dot
    scale_two = lax.rsqrt(resid_sq / width + EPS)
    residual_f = start_part + lifted * branch_scale
    residual = residual_f.astype(bf16).astype(f32)
    rows_in[0] = (residual_f * scale_two * gain_two).astype(bf16)
    row_copies = [None] * ep_count
    for p in range(1, ep_count):
        row_copies[p] = ep_copy(rows_in.at[0], rows_in.at[p], p)
    mix_gate = jax.nn.sigmoid(scale_two * gate_dot)
    mg_send[0:1, 0:seqs] = to_row(mix_gate)
    mg_copies = [ep_copy(mg_send, mg_recv.at[p], p) for p in range(1, ep_count)]
    mine = lax.broadcasted_iota(jnp.int32, (experts, seqs), 0) == ep
    wanted = (lax.broadcasted_iota(jnp.int32, (capacity, seqs), 0) + 1).astype(f32)
    wide_row = lax.broadcasted_iota(jnp.int32, (seqs, chunk_rows), 0)
    wide_column = lax.broadcasted_iota(jnp.int32, (seqs, chunk_rows), 1)
    arrive(info_copies)
    placings = []
    shares = []
    for k in range(chunks):
        blocks = []
        for q in range(per):
            p = k * per + q
            if p == 0:
                codes, portion = info_send[0], info_send[1]
            else:
                codes, portion = info_recv[p, 0], info_recv[p, 1]
            code = jnp.sum(jnp.where(mine, codes[:, 0:seqs], 0.0), axis=0, keepdims=True)
            one = jnp.where(code == wanted, 1.0, 0.0).astype(bf16)
            moved = jnp.where(wide_row + q * seqs == wide_column, 1.0, 0.0).astype(bf16)
            blocks.append(jnp.dot(one, moved, preferred_element_type=f32).astype(bf16))
            shares.append(to_column(jnp.sum(jnp.where(mine, portion[:, 0:seqs], 0.0), axis=0, keepdims=True)))
        placings.append(jnp.concatenate(blocks, axis=0))

    def xin_at(k):
        return lambda i: xin.at[i, pl.ds(k * chunk_slots, chunk_slots)]

    def pre_at(k):
        return lambda i: pre_send.at[k, i]

    def of(ref, k):
        return lambda j: ref.at[k, j]

    def hid_at(k):
        return lambda i: hid.at[k, i]

    xin_copies = []
    pre_copies = []
    hid_copies = []

    def chunk_in(k):
        for p in range(k * per, (k + 1) * per):
            if p > 0:
                row_copies[p].wait_recv()
        rows = rows_in[k * per : (k + 1) * per].reshape(chunk_rows, part)
        xin[tp, k * chunk_slots : (k + 1) * chunk_slots] = jnp.dot(
            placings[k], rows, preferred_element_type=f32
        ).astype(bf16)
        xin_copies.append(gather_start(xin_at(k)))
        for i, weight in enumerate((dgt, dut)):
            made = jnp.dot(rows, weight[...], preferred_element_type=f32).astype(bf16)
            for t in range(tp_count):
                pre_send[k, t, i] = made[t * quarter : (t + 1) * quarter]
        pre_copies.append(scatter_pair(pre_at(k), of(pre_one, k)))

    def pre_cross(k):
        scatter_cross(pre_at(k), of(pre_one, k), of(pre_mid, k), of(pre_two, k), pre_copies[k])

    def pre_done(k):
        pre = scatter_sum(pre_at(k), of(pre_one, k), of(pre_two, k), pre_copies[k])
        hid[k, tp] = (jax.nn.silu(pre[0]) * pre[1]).astype(bf16)
        hid_copies.append(gather_start(hid_at(k)))

    def xin_relay(k):
        gather_relay(xin_at(k), xin_copies[k])

    def hid_relay(k):
        gather_relay(hid_at(k), hid_copies[k])

    sums_of = [None, None]

    def expert_in(source):
        for i, weight in enumerate((eg, eu)):
            made = jnp.dot(xin[source], weight[columns(source), :], preferred_element_type=f32)
            sums_of[i] = made if sums_of[i] is None else sums_of[i] + made

    chunk_in(0)
    pre_cross(0)
    for k in range(1, chunks):
        chunk_in(k)
        if k >= 2:
            pre_cross(k - 1)
    arrive(mg_copies)
    gates = [mix_gate] + [to_column(mg_recv[p, 0:1, 0:seqs]) for p in range(1, ep_count)]
    loads[2].wait()
    loads[3].wait()
    expert_in(tp)
    pre_cross(chunks - 1)
    for k in range(chunks - 1):
        xin_relay(k)
    pre_done(0)
    for k in range(chunks):
        xin_copies[k][groups - 1].wait_recv()
    expert_in(pair)
    xin_relay(chunks - 1)
    pre_done(1)
    for d in range(1, groups):
        expert_in(behind(d))
    pre_done(2)
    for d in range(1, groups):
        for k in range(chunks):
            xin_copies[k][groups - 1 + d].wait_recv()
        expert_in(behind(d) + 1 - 2 * parity)
    hidden_units = (jax.nn.silu(sums_of[0]) * sums_of[1]).astype(bf16)

    loads[4].wait()
    eo_copies = [None] * chunks
    turn = list(range(chunks))[::-1]

    def piece_of(ref, k):
        return lambda i: ref.at[i, pl.ds(k * chunk_slots, chunk_slots)]

    def expert_down(t):
        eo_send[t] = jnp.dot(hidden_units, ed[:, columns(t)], preferred_element_type=f32).astype(bf16)

    for k in range(3, chunks):
        pre_done(k)
    for j in range(groups):
        expert_down(j * 2 + 1 - parity)
    for k in turn:
        eo_copies[k] = scatter_pair(piece_of(eo_send, k), piece_of(eo_one, k))
    for j in range(groups):
        expert_down(j * 2 + parity)
    hid_relay(0)
    for k in turn:
        scatter_cross(
            piece_of(eo_send, k), piece_of(eo_one, k), piece_of(eo_mid, k), piece_of(eo_two, k), eo_copies[k]
        )
    for k in range(1, chunks):
        hid_relay(k)
    loads[5].wait()
    units = hid.shape[3]
    for k in range(chunks):
        arrive(hid_copies[k][groups - 1 :])
    dense_out[...] = jnp.dot(
        hid[...].reshape(ep_count * seqs, units), dd[...], preferred_element_type=f32
    )
    for p in range(ep_count):
        rows = slice(p * seqs, (p + 1) * seqs)
        dense_out[rows] = gates[p] * dense_out[rows]
    relayed = range(chunks // 2, chunks)
    c_copies = {}
    parts = {}
    near = {}
    first_dims = (((0,), (0,)), ((), ()))

    def c_cross(k):
        for p in range(k * per, (k + 1) * per, 2):
            near[p].wait_recv()
            c_send[p] = (parts[p] + c_recv[p + 1].astype(f32)).astype(bf16)
            c_copies[p] = ep_copy(c_send.at[p], c_recv.at[p], p)

    for k in turn:
        total = scatter_sum(piece_of(eo_send, k), piece_of(eo_one, k), piece_of(eo_two, k), eo_copies[k])
        total = total.astype(bf16)
        picked = lax.dot_general(placings[k], total, first_dims, preferred_element_type=f32)
        for q in list(range(per))[::-1]:
            p = k * per + q
            combined = (
                dense_out[p * seqs : (p + 1) * seqs] + shares[p] * picked[q * seqs : (q + 1) * seqs]
            )
            if p == 0:
                parts[p] = combined
            elif k in relayed and p % 2 == 0:
                parts[p] = combined
            else:
                c_send[p] = combined.astype(bf16)
                if k in relayed:
                    near[p - 1] = ep_copy(c_send.at[p], c_recv.at[p], 1)
                else:
                    c_copies[p] = ep_copy(c_send.at[p], c_recv.at[p], p)
        if k == 0:
            for late in reversed(relayed):
                c_cross(late)
    ffn = parts[0]
    for p in sorted(c_copies):
        c_copies[p].wait_recv()
        ffn = ffn + c_recv[p].astype(f32)
    fs_send[0:1, 0:seqs] = to_row(jnp.sum(ffn * ffn, axis=1, keepdims=True))
    final_copies = tp_all(lambda peer: fs_send, fs_recv.at[tp])
    scaled = gain_three * ffn
    squares = fs_send[...]
    arrive(final_copies)
    for d in range(1, tp_count):
        squares = squares + fs_recv[from_tp(d)]
    scale = to_column(lax.rsqrt(squares[0:1, 0:seqs] / width + EPS))
    out_ref[...] = (residual + scaled * scale).astype(bf16)
    for copy in started:
        copy.wait_send()


def tail(
    terms, hidden, norm_gains, dense_mix, routes, route_scores, weights
):
    tp_count = lax.axis_size("tp")
    ep_count = lax.axis_size("ep")
    seqs, width = hidden.shape
    part = width // tp_count
    expert_gate, expert_up, expert_down, dense_gate, dense_up, dense_down = weights
    units = expert_gate.shape[2]
    dense_gate, dense_up = dense_gate.T, dense_up.T
    dense_units = dense_gate.shape[0]
    top = routes.shape[1]
    experts = ep_count * expert_gate.shape[0]
    limit = 2 * seqs * top // ep_count
    capacity = -(-limit // 16) * 16
    chunks = 4
    rows_all = ep_count * seqs
    quarter = rows_all // chunks // tp_count
    groups = tp_count // 2
    lanes = -(-seqs // 128) * 128
    f32, bf16 = jnp.float32, jnp.bfloat16
    vmem = pl.BlockSpec(memory_space=pltpu.VMEM)
    hbm = pl.BlockSpec(memory_space=pl.ANY)
    slots = ep_count * capacity
    tp_copies = 3 * (tp_count - 1) + 4 * chunks * (2 * groups - 1)
    ep_copies = 4 * (ep_count - 1)
    sums = -(-6 * seqs // 128) * 128
    piece = pltpu.VMEM((chunks, groups, 2, quarter, dense_units), bf16)
    return pl.pallas_call(
        functools.partial(tail_kernel, tp_count, ep_count, capacity, chunks),
        out_shape=jax.ShapeDtypeStruct((seqs, part), bf16),
        in_specs=[hbm] * 12,
        out_specs=vmem,
        scratch_shapes=[
            pltpu.VMEM((tp_count, seqs, part), bf16),
            pltpu.VMEM((seqs, part), bf16),
            pltpu.VMEM((norm_gains.shape[0], part), f32),
            pltpu.VMEM((1, part), f32),
            pltpu.VMEM((top, seqs), jnp.int32),
            pltpu.VMEM((top, seqs), f32),
            pltpu.VMEM((width, units), bf16),
            pltpu.VMEM((width, units), bf16),
            pltpu.VMEM((units, width), bf16),
            pltpu.VMEM(dense_gate.shape, bf16),
            pltpu.VMEM(dense_up.shape, bf16),
            pltpu.VMEM(dense_down.shape, bf16),
            pltpu.VMEM(dense_gate.shape[::-1], bf16),
            pltpu.VMEM(dense_up.shape[::-1], bf16),
            pltpu.VMEM((tp_count, seqs, part), bf16),
            pltpu.VMEM((1, sums), f32),
            pltpu.VMEM((tp_count, 1, sums), f32),
            pltpu.VMEM((1, lanes), f32),
            pltpu.VMEM((tp_count, 1, lanes), f32),
            pltpu.VMEM((2, experts, lanes), f32),
            pltpu.VMEM((ep_count, 2, experts, lanes), f32),
            pltpu.VMEM((1, lanes), f32),
            pltpu.VMEM((ep_count, 1, lanes), f32),
            pltpu.VMEM((ep_count, seqs, part), bf16),
            pltpu.VMEM((tp_count, slots, part), bf16),
            pltpu.VMEM((chunks, tp_count, 2, quarter, dense_units), bf16),
            piece,
            piece,
            piece,
            pltpu.VMEM((chunks, tp_count, quarter, dense_units), bf16),
            pltpu.VMEM((rows_all, part), f32),
            pltpu.VMEM((tp_count, slots, part), bf16),
            pltpu.VMEM((groups, slots, part), bf16),
            pltpu.VMEM((groups, slots, part), bf16),
            pltpu.VMEM((groups, slots, part), bf16),
            pltpu.VMEM((ep_count, seqs, part), bf16),
            pltpu.VMEM((ep_count, seqs, part), bf16),
            pltpu.SemaphoreType.DMA((6,)),
            pltpu.SemaphoreType.DMA((6,)),
            pltpu.SemaphoreType.REGULAR,
            pltpu.SemaphoreType.REGULAR,
            pltpu.SemaphoreType.DMA((tp_copies,)),
            pltpu.SemaphoreType.DMA((tp_copies,)),
            pltpu.SemaphoreType.DMA((ep_copies,)),
            pltpu.SemaphoreType.DMA((ep_copies,)),
        ],
        compiler_params=pltpu.CompilerParams(
            collective_id=0, has_side_effects=True, vmem_limit_bytes=67043328
        ),
        name="tail",
    )(
        terms,
        hidden,
        norm_gains,
        dense_mix.reshape(1, width),
        routes.T,
        route_scores.T,
        expert_gate,
        expert_up,
        expert_down,
        dense_gate,
        dense_up,
        dense_down,
    )


def local(
    hidden,
    norm_gains,
    w_query,
    w_key,
    w_value,
    w_outgate,
    w_input_gate,
    w_forget_gate,
    forget_bias,
    w_mix_out,
    state_matrix,
    state_norm,
    state_max,
    routes,
    route_scores,
    expert_gate,
    expert_up,
    expert_down,
    dense_gate,
    dense_up,
    dense_down,
    dense_mix,
):
    terms, new_matrix, new_norm, new_max = front(
        hidden,
        norm_gains,
        (w_input_gate, w_forget_gate),
        forget_bias,
        state_norm,
        state_max,
        (w_query, w_key, w_value, w_outgate, w_mix_out),
        state_matrix,
    )
    new_hidden = tail(
        terms,
        hidden,
        norm_gains,
        dense_mix,
        routes,
        route_scores,
        (expert_gate, expert_up, expert_down, dense_gate, dense_up, dense_down),
    )
    return (new_hidden, new_matrix, new_norm, new_max)


def solution(mesh):
    placed = (
        P("ep", None),
        P(),
        P(None, "tp"),
        P(None, "tp"),
        P(None, "tp"),
        P(None, "tp"),
        P(),
        P(),
        P(),
        P("tp", None),
        P("ep", "tp", None, None),
        P("ep", "tp", None),
        P("ep", "tp"),
        P("ep", None),
        P("ep", None),
        P("ep", None, "tp"),
        P("ep", None, "tp"),
        P("ep", "tp", None),
        P("tp", "ep"),
        P("tp", "ep"),
        P("ep", "tp"),
        P(),
    )
    return jax.shard_map(
        local,
        mesh=mesh,
        in_specs=placed,
        out_specs=(P("ep", "tp"), P("ep", "tp", None, None), P("ep", "tp", None), P("ep", "tp")),
        check_vma=False,
    )
```

```python
import functools

import jax
import jax.numpy as jnp
from jax import lax
from jax.experimental import pallas as pl
from jax.experimental.pallas import tpu as pltpu
from jax.sharding import PartitionSpec as P

EPS = 1e-06


def front_kernel(
    hidden_hbm,
    gains_hbm,
    in_hbm,
    forget_hbm,
    bias_hbm,
    norm_hbm,
    max_hbm,
    wq_hbm,
    wk_hbm,
    wv_hbm,
    wo_hbm,
    wm_hbm,
    state_hbm,
    terms_hbm,
    matrix_hbm,
    new_norm_hbm,
    new_max_ref,
    wq,
    wk,
    wv,
    wo,
    wm,
    hidden,
    gains,
    in_weight,
    forget_weight,
    bias,
    norm,
    top,
    state,
    numer,
    terms,
    new_norms,
    s_sem,
    w_sem,
    in_sem,
    out_sem,
    end_sem,
):
    tp = lax.axis_index("tp")
    f32, bf16 = jnp.float32, jnp.bfloat16
    seqs = hidden.shape[0]
    heads, head = state.shape[1], state.shape[2]
    chunks = in_sem.shape[0]
    step = seqs // chunks
    smalls = []
    for i, (src, dst) in enumerate(
        (
            (hidden_hbm, hidden),
            (gains_hbm, gains),
            (in_hbm, in_weight),
            (forget_hbm, forget_weight),
            (bias_hbm, bias),
            (max_hbm, top),
            (norm_hbm, norm),
        )
    ):
        smalls.append(pltpu.make_async_copy(src, dst, s_sem.at[i]))
    for small in smalls[:4]:
        small.start()
    loads = []
    for i, (src, dst) in enumerate(((wk_hbm, wk), (wq_hbm, wq), (wv_hbm, wv), (wo_hbm, wo), (wm_hbm, wm))):
        loads.append(pltpu.make_async_copy(src, dst, w_sem.at[i]))
    fetches = []
    for c in range(chunks):
        rows = pl.ds(c * step, step)
        fetches.append(pltpu.make_async_copy(state_hbm.at[rows], state.at[rows], in_sem.at[c]))
    for load in loads[:3]:
        load.start()
    for small in smalls[4:]:
        small.start()
    for small in smalls[:4]:
        small.wait()
    for fetch in fetches:
        fetch.start()
    for load in loads[3:]:
        load.start()

    start = hidden[...].astype(f32)
    scale = lax.rsqrt(jnp.mean(start * start, axis=1, keepdims=True) + EPS)
    normed = (start * scale * gains[0:1, :]).astype(bf16)
    last = (((1,), (1,)), ((), ()))
    in_all = lax.dot_general(normed, in_weight[...], last, preferred_element_type=f32)
    forget_all = lax.dot_general(normed, forget_weight[...], last, preferred_element_type=f32)
    column = lax.broadcasted_iota(jnp.int32, in_all.shape, 1)
    here = lax.broadcasted_iota(jnp.int32, (seqs, seqs), 0)
    there = lax.broadcasted_iota(jnp.int32, (seqs, seqs), 1)
    projected = []
    for i, weight in enumerate((wk, wq, wv)):
        loads[i].wait()
        product = jnp.dot(normed, weight[...], preferred_element_type=f32)
        projected.append(product.astype(bf16).astype(f32))
    keys, query, values = projected
    for small in smalls[4:]:
        small.wait()
    forget_all = forget_all + bias[...]
    forget_all = jnp.minimum(forget_all, 0.0) - jnp.log(1.0 + jnp.exp(-jnp.abs(forget_all)))
    keeps = []
    bounds = []
    outers = []
    turns = []
    for h in range(heads):
        span = slice(h * head, (h + 1) * head)
        mine = column == tp * heads + h
        in_gate = jnp.sum(jnp.where(mine, in_all, 0.0), axis=1, keepdims=True)
        log_forget = jnp.sum(jnp.where(mine, forget_all, 0.0), axis=1, keepdims=True)
        before = jnp.sum(jnp.where(here == there, top[h : h + 1, :], 0.0), axis=1, keepdims=True)
        carried = log_forget + before
        new_max = jnp.maximum(carried, in_gate)
        keep = jnp.exp(carried - new_max)
        write = jnp.exp(in_gate - new_max) * head ** (-0.5)
        new_max_ref[h : h + 1, :] = jnp.sum(
            jnp.where(here == there, new_max, 0.0), axis=0, keepdims=True
        )
        new_norm = keep * norm[:, h, :] + write * keys[:, span]
        new_norms[:, h, :] = new_norm
        denom = jnp.sum(query[:, span] * new_norm, axis=1, keepdims=True)
        bounds.append(jnp.maximum(jnp.abs(denom), jnp.exp(-new_max)))
        keeps.append(jnp.broadcast_to(keep, (seqs, head)))
        added = write * values[:, span]
        high = added.astype(bf16).astype(f32)
        middle = (added - high).astype(bf16).astype(f32)
        low = (added - high - middle).astype(bf16).astype(f32)
        outers.append(jnp.concatenate([high, middle, low, jnp.zeros_like(low)], axis=0))
        turned = jnp.concatenate([keys[:, span]] * 3 + [query[:, span]], axis=0).T
        turns.append((turned, turned.astype(bf16)))
    norm_store = pltpu.make_async_copy(new_norms, new_norm_hbm, end_sem.at[0])
    norm_store.start()
    from_seq = lax.rem(lax.broadcasted_iota(jnp.int32, outers[0].shape, 0), seqs)
    stores = []
    for c in range(chunks):
        fetches[c].wait()
        for s in range(c * step, (c + 1) * step, 2):
            for h in range(heads):
                turned, turned_half = turns[h]
                picked = [jnp.where(from_seq == s + i, outers[h], 0.0).astype(bf16) for i in range(2)]
                written = jnp.dot(
                    turned_half, jnp.concatenate(picked, axis=1), preferred_element_type=f32
                )
                for i in range(2):
                    at = 3 * seqs + s + i
                    query_col = turned[:, at : at + 1]
                    new = (
                        keeps[h][s + i : s + i + 1, :] * state[s + i, h]
                        + written[:, i * head : (i + 1) * head]
                    )
                    state[s + i, h] = new
                    numer[h, s + i : s + i + 1, :] = jnp.sum(query_col * new, axis=0, keepdims=True)
        rows = pl.ds(c * step, step)
        stores.append(pltpu.make_async_copy(state.at[rows], matrix_hbm.at[rows], out_sem.at[c]))
        stores[c].start()
    loads[3].wait()
    gate = jnp.dot(normed, wo[...], preferred_element_type=f32).astype(bf16).astype(f32)
    mixed = []
    for h in range(heads):
        span = slice(h * head, (h + 1) * head)
        mixed.append((jax.nn.sigmoid(gate[:, span]) * (numer[h] / bounds[h])).astype(bf16))
    mixed = jnp.concatenate(mixed, axis=1)
    loads[4].wait()
    part = terms.shape[2]
    for t in range(terms.shape[0]):
        terms[t] = jnp.dot(
            mixed, wm[:, t * part : (t + 1) * part], preferred_element_type=f32
        ).astype(bf16)
    terms_store = pltpu.make_async_copy(terms, terms_hbm, end_sem.at[1])
    terms_store.start()
    for store in stores + [norm_store, terms_store]:
        store.wait()


def front(hidden, norm_gains, gate_weights, forget_bias, state_norm, state_max, weights, state_matrix):
    tp_count = lax.axis_size("tp")
    seqs, width = hidden.shape
    heads, head = state_matrix.shape[1], state_matrix.shape[2]
    f32, bf16 = jnp.float32, jnp.bfloat16
    chunks = 4
    vmem = pl.BlockSpec(memory_space=pltpu.VMEM)
    hbm = pl.BlockSpec(memory_space=pl.ANY)
    smalls = (
        hidden,
        norm_gains,
        gate_weights[0].T,
        gate_weights[1].T,
        forget_bias.reshape(1, -1),
        state_norm,
        state_max.T,
    )
    terms, matrix, norm, top = pl.pallas_call(
        front_kernel,
        out_shape=(
            jax.ShapeDtypeStruct((tp_count, seqs, width // tp_count), bf16),
            jax.ShapeDtypeStruct(state_matrix.shape, f32),
            jax.ShapeDtypeStruct(state_norm.shape, f32),
            jax.ShapeDtypeStruct((heads, seqs), f32),
        ),
        in_specs=[hbm] * 13,
        out_specs=(hbm, hbm, hbm, vmem),
        scratch_shapes=[pltpu.VMEM(weight.shape, bf16) for weight in weights]
        + [pltpu.VMEM(small.shape, small.dtype) for small in smalls]
        + [
            pltpu.VMEM(state_matrix.shape, f32),
            pltpu.VMEM((heads, seqs, head), f32),
            pltpu.VMEM((tp_count, seqs, width // tp_count), bf16),
            pltpu.VMEM(state_norm.shape, f32),
            pltpu.SemaphoreType.DMA((7,)),
            pltpu.SemaphoreType.DMA((5,)),
            pltpu.SemaphoreType.DMA((chunks,)),
            pltpu.SemaphoreType.DMA((chunks,)),
            pltpu.SemaphoreType.DMA((2,)),
        ],
        compiler_params=pltpu.CompilerParams(vmem_limit_bytes=67043328),
        name="front",
    )(*smalls, *weights, state_matrix)
    return terms, matrix, norm, top.T


MESH = pl.DeviceIdType.MESH


def tail_kernel(
    tp_count,
    ep_count,
    capacity,
    chunks,
    terms_hbm,
    hidden_hbm,
    gains_hbm,
    mix_hbm,
    routes_hbm,
    scores_hbm,
    eg_hbm,
    eu_hbm,
    ed_hbm,
    dg_hbm,
    du_hbm,
    dd_hbm,
    out_ref,
    terms,
    start_in,
    gains,
    mix,
    routes,
    scores,
    eg,
    eu,
    ed,
    dg,
    du,
    dd,
    dgt,
    dut,
    br_recv,
    st_send,
    st_recv,
    fs_send,
    fs_recv,
    info_send,
    info_recv,
    mg_send,
    mg_recv,
    rows_in,
    xin,
    pre_send,
    pre_one,
    pre_mid,
    pre_two,
    hid,
    dense_out,
    eo_send,
    eo_one,
    eo_mid,
    eo_two,
    c_send,
    c_recv,
    s_sem,
    w_sem,
    join_sem,
    go_sem,
    tp_send,
    tp_recv,
    ep_send,
    ep_recv,
):
    tp = lax.axis_index("tp")
    ep = lax.axis_index("ep")
    seqs, part = start_in.shape
    width = part * tp_count
    per = ep_count // chunks
    chunk_rows = per * seqs
    chunk_slots = per * capacity
    quarter = chunk_rows // tp_count
    first = pl.multiple_of(tp * part, part)
    f32, bf16 = jnp.float32, jnp.bfloat16

    own = pl.ds(first, part)
    smalls = []
    for i, (src, dst) in enumerate(
        (
            (terms_hbm, terms),
            (hidden_hbm.at[:, own], start_in),
            (gains_hbm.at[:, own], gains),
            (mix_hbm.at[:, own], mix),
            (routes_hbm, routes),
            (scores_hbm, scores),
        )
    ):
        load = pltpu.make_async_copy(src, dst, s_sem.at[i])
        load.start()
        smalls.append(load)

    def partner(p):
        other = ep
        bit = 1
        while bit < ep_count:
            if p & bit:
                other = other + bit * (1 - 2 * lax.rem(ep // bit, 2))
            bit *= 2
        return other

    barrier = pltpu.get_barrier_semaphore()
    for d in range(1, tp_count):
        peer = lax.rem(tp + d, tp_count)

        @pl.when(peer != 0)
        def _(peer=peer):
            pl.semaphore_signal(barrier, inc=1, device_id={"tp": peer}, device_id_type=MESH)

    loads = []
    for i, (src, dst) in enumerate(
        ((dg_hbm, dg), (du_hbm, du), (eg_hbm.at[0], eg), (eu_hbm.at[0], eu), (ed_hbm.at[0], ed), (dd_hbm, dd))
    ):
        load = pltpu.make_async_copy(src, dst, w_sem.at[i])
        load.start()
        loads.append(load)

    groups = tp_count // 2
    parity = lax.rem(tp, 2)
    group = tp // 2
    pair = tp + 1 - 2 * parity
    started = []
    tp_next = [0]
    ep_next = [0]

    def tp_copy(src, dst, peer):
        at = tp_next[0]
        tp_next[0] += 1
        copy = pltpu.make_async_remote_copy(
            src_ref=src,
            dst_ref=dst,
            send_sem=tp_send.at[at],
            recv_sem=tp_recv.at[at],
            device_id={"tp": peer},
            device_id_type=MESH,
        )
        copy.start()
        started.append(copy)
        return copy

    def ep_copy(src, dst, p):
        at = ep_next[0]
        ep_next[0] += 1
        copy = pltpu.make_async_remote_copy(
            src_ref=src,
            dst_ref=dst,
            send_sem=ep_send.at[at],
            recv_sem=ep_recv.at[at],
            device_id={"ep": partner(p)},
            device_id_type=MESH,
        )
        copy.start()
        started.append(copy)
        return copy

    def tp_all(src_of, dst):
        made = []
        for d in range(1, tp_count):
            peer = lax.rem(tp + d, tp_count)
            made.append(tp_copy(src_of(peer), dst, peer))
        return made

    def ahead(d):
        return lax.rem(group + d, groups) * 2 + parity

    def behind(d):
        return lax.rem(group + groups - d, groups) * 2 + parity

    def gather_start(at):
        made = [tp_copy(at(tp), at(tp), ahead(d)) for d in range(1, groups)]
        made.append(tp_copy(at(tp), at(tp), pair))
        return made

    def gather_relay(at, made):
        for d in range(1, groups):
            made[d - 1].wait_recv()
            made.append(tp_copy(at(behind(d)), at(behind(d)), pair))

    def other(d):
        return lax.rem(group + d, groups)

    def scatter_pair(at, one, d):
        return tp_copy(at(other(d) * 2 + 1 - parity), one(other(d)), pair)

    def scatter_cross(at, one, mid, two, made):
        for d in range(1, groups):
            j = other(d)
            made[d].wait_recv()
            mid(j)[...] = (at(ahead(d))[...].astype(f32) + one(j)[...].astype(f32)).astype(bf16)
            made.append(tp_copy(mid(j), two(group), ahead(d)))

    def scatter_sum(at, one, two, made):
        made[0].wait_recv()
        total = at(tp)[...].astype(f32) + one(group)[...].astype(f32)
        for d in range(1, groups):
            made[groups + d - 1].wait_recv()
            total = total + two(lax.rem(group + groups - d, groups))[...].astype(f32)
        return total

    def arrive(copies):
        for copy in copies:
            copy.wait_recv()

    def from_tp(d):
        return lax.rem(tp + tp_count - d, tp_count)

    def columns(peer):
        return pl.ds(pl.multiple_of(peer * part, part), part)

    for ref in (fs_send, mg_send, info_send):
        ref[...] = jnp.zeros(ref.shape, f32)
    here = lax.broadcasted_iota(jnp.int32, (seqs, seqs), 0)
    there = lax.broadcasted_iota(jnp.int32, (seqs, seqs), 1)
    diagonal = here == there

    def to_row(column):
        return jnp.sum(jnp.where(diagonal, column, 0.0), axis=0, keepdims=True)

    def to_column(row):
        return jnp.sum(jnp.where(diagonal, row, 0.0), axis=1, keepdims=True)

    for load in smalls:
        load.wait()

    @pl.when(tp != 0)
    def _():
        pl.semaphore_wait(barrier, tp_count - 1)
        pl.semaphore_signal(join_sem, inc=1, device_id={"tp": 0}, device_id_type=MESH)

    @pl.when(tp == 0)
    def _():
        pl.semaphore_wait(join_sem, tp_count - 1)
        for p in range(1, ep_count):
            pl.semaphore_signal(barrier, inc=1, device_id={"ep": partner(p)}, device_id_type=MESH)

    branch_copies = tp_all(lambda peer: terms.at[peer], br_recv.at[tp])

    top = routes.shape[0]
    experts = info_send.shape[1]
    name = lax.broadcasted_iota(jnp.int32, (experts, seqs), 0)
    hits = [routes[k : k + 1, :] == name for k in range(top)]
    named = hits[0]
    for k in range(1, top):
        named = jnp.logical_or(named, hits[k])
    named = jnp.where(named, 1.0, 0.0)
    before = jnp.where(here < there, 1.0, 0.0).astype(bf16)
    rank = jnp.dot(named.astype(bf16), before, preferred_element_type=f32) + 1.0
    score_sum = scores[0:1, :]
    for k in range(1, top):
        score_sum = score_sum + scores[k : k + 1, :]
    share = jnp.zeros((experts, seqs), f32)
    for k in range(top):
        share = share + jnp.where(hits[k], scores[k : k + 1, :] / score_sum, 0.0)
    info_send[0, :, 0:seqs] = named * rank
    info_send[1, :, 0:seqs] = share

    start_part = start_in[...].astype(f32)
    gain_one = gains[1:2, :]
    gain_two = gains[2:3, :]
    gain_three = gains[3:4, :]
    mix_weight = gain_two * mix[...]
    start_sq = jnp.sum(start_part * start_part, axis=1, keepdims=True)
    start_dot = jnp.sum(start_part * mix_weight, axis=1, keepdims=True)
    branch = terms[tp].astype(f32)
    loads[0].wait()
    dgt[...] = dg[...].T
    arrive(branch_copies)
    for d in range(1, tp_count):
        branch = branch + br_recv[from_tp(d)].astype(f32)
    branch = branch.astype(bf16).astype(f32)
    lifted = gain_one * branch
    lanes = st_send.shape[1]
    lane = lax.broadcasted_iota(jnp.int32, (seqs, lanes), 1)
    place_of = lax.broadcasted_iota(jnp.int32, (seqs, lanes), 0)

    def pack(values):
        made = jnp.zeros((seqs, lanes), f32)
        for i, value in enumerate(values):
            made = jnp.where(lane == place_of + i * seqs, value, made)
        return jnp.sum(made, axis=0, keepdims=True)

    def unpack(row, i):
        return jnp.sum(jnp.where(lane == place_of + i * seqs, row, 0.0), axis=1, keepdims=True)

    packed = pack(
        (
            jnp.sum(branch * branch, axis=1, keepdims=True),
            start_sq,
            jnp.sum(start_part * lifted, axis=1, keepdims=True),
            jnp.sum(lifted * lifted, axis=1, keepdims=True),
            start_dot,
            jnp.sum(lifted * mix_weight, axis=1, keepdims=True),
        )
    )
    st_send[...] = packed
    stat_copies = tp_all(lambda peer: st_send, st_recv.at[tp])

    @pl.when(tp == 0)
    def _():
        pl.semaphore_wait(barrier, ep_count - 1)
        for t in range(1, tp_count):
            pl.semaphore_signal(go_sem, inc=1, device_id={"tp": t}, device_id_type=MESH)

    @pl.when(tp != 0)
    def _():
        pl.semaphore_wait(go_sem, 1)

    info_copies = [ep_copy(info_send, info_recv.at[p], p) for p in range(1, ep_count)]
    loads[1].wait()
    dut[...] = du[...].T
    arrive(stat_copies)
    for d in range(1, tp_count):
        packed = packed + st_recv[from_tp(d)]
    branch_sq, start_sq, cross_sum, lifted_sq, start_dot, lifted_dot = (
        unpack(packed, i) for i in range(6)
    )
    branch_scale = lax.rsqrt(branch_sq / width + EPS)
    resid_sq = start_sq + 2.0 * branch_scale * cross_sum + branch_scale * branch_scale * lifted_sq
    gate_dot = start_dot + branch_scale * lifted_dot
    scale_two = lax.rsqrt(resid_sq / width + EPS)
    residual_f = start_part + lifted * branch_scale
    residual = residual_f.astype(bf16).astype(f32)
    rows_in[0] = (residual_f * scale_two * gain_two).astype(bf16)
    row_copies = [None] * ep_count
    for p in list(range(1, ep_count)):
        row_copies[p] = ep_copy(rows_in.at[0], rows_in.at[p], p)
    mix_gate = jax.nn.sigmoid(scale_two * gate_dot)
    mg_send[0:1, 0:seqs] = to_row(mix_gate)
    mg_copies = [ep_copy(mg_send, mg_recv.at[p], p) for p in range(1, ep_count)]
    mine = lax.broadcasted_iota(jnp.int32, (experts, seqs), 0) == ep
    wanted = (lax.broadcasted_iota(jnp.int32, (capacity, seqs), 0) + 1).astype(f32)
    wide_row = lax.broadcasted_iota(jnp.int32, (seqs, chunk_rows), 0)
    wide_column = lax.broadcasted_iota(jnp.int32, (seqs, chunk_rows), 1)
    arrive(info_copies)
    placings = []
    shares = []
    for k in range(chunks):
        blocks = []
        for q in range(per):
            p = k * per + q
            if p == 0:
                codes, portion = info_send[0], info_send[1]
            else:
                codes, portion = info_recv[p, 0], info_recv[p, 1]
            code = jnp.sum(jnp.where(mine, codes[:, 0:seqs], 0.0), axis=0, keepdims=True)
            one = jnp.where(code == wanted, 1.0, 0.0).astype(bf16)
            moved = jnp.where(wide_row + q * seqs == wide_column, 1.0, 0.0).astype(bf16)
            blocks.append(jnp.dot(one, moved, preferred_element_type=f32).astype(bf16))
            shares.append(to_column(jnp.sum(jnp.where(mine, portion[:, 0:seqs], 0.0), axis=0, keepdims=True)))
        placings.append(jnp.concatenate(blocks, axis=0))

    def xin_at(k):
        return lambda i: xin.at[i, pl.ds(k * chunk_slots, chunk_slots)]

    def pre_at(k):
        return lambda i: pre_send.at[k, i]

    def of(ref, k):
        return lambda j: ref.at[k, j]

    def hid_at(k):
        return lambda i: hid.at[k, i]

    xin_copies = []
    pre_copies = []
    hid_copies = []

    def chunk_in(k):
        for p in range(k * per, (k + 1) * per):
            if p > 0:
                row_copies[p].wait_recv()
        rows = rows_in[k * per : (k + 1) * per].reshape(chunk_rows, part)
        xin[tp, k * chunk_slots : (k + 1) * chunk_slots] = jnp.dot(
            placings[k], rows, preferred_element_type=f32
        ).astype(bf16)
        xin_copies.append(gather_start(xin_at(k)))
        for i, weight in enumerate((dgt, dut)):
            made = jnp.dot(rows, weight[...], preferred_element_type=f32).astype(bf16)
            for t in range(tp_count):
                pre_send[k, t, i] = made[t * quarter : (t + 1) * quarter]
        far_first = list(range(1, groups)) + [0]
        made = {d: scatter_pair(pre_at(k), of(pre_one, k), d) for d in far_first}
        pre_copies.append([made[d] for d in range(groups)])

    def pre_cross(k):
        scatter_cross(pre_at(k), of(pre_one, k), of(pre_mid, k), of(pre_two, k), pre_copies[k])

    def pre_done(k):
        pre = scatter_sum(pre_at(k), of(pre_one, k), of(pre_two, k), pre_copies[k])
        hid[k, tp] = (jax.nn.silu(pre[0]) * pre[1]).astype(bf16)
        hid_copies.append(gather_start(hid_at(k)))

    def xin_relay(k):
        gather_relay(xin_at(k), xin_copies[k])

    def hid_relay(k):
        gather_relay(hid_at(k), hid_copies[k])

    sums_of = [None, None]

    def expert_in(source):
        for i, weight in enumerate((eg, eu)):
            made = jnp.dot(xin[source], weight[columns(source), :], preferred_element_type=f32)
            sums_of[i] = made if sums_of[i] is None else sums_of[i] + made

    chunk_in(0)
    pre_cross(0)
    for k in range(1, chunks):
        chunk_in(k)
        if k >= 2:
            pre_cross(k - 1)
    arrive(mg_copies)
    gates = [mix_gate] + [to_column(mg_recv[p, 0:1, 0:seqs]) for p in range(1, ep_count)]
    loads[2].wait()
    loads[3].wait()
    expert_in(tp)
    pre_cross(chunks - 1)
    for k in range(chunks - 1):
        xin_relay(k)
    pre_done(0)
    for k in range(chunks):
        xin_copies[k][groups - 1].wait_recv()
    expert_in(pair)
    xin_relay(chunks - 1)
    pre_done(1)
    for d in range(1, groups):
        expert_in(behind(d))
    pre_done(2)
    for d in range(1, groups):
        for k in range(chunks):
            xin_copies[k][groups - 1 + d].wait_recv()
        expert_in(behind(d) + 1 - 2 * parity)
    hidden_units = (jax.nn.silu(sums_of[0]) * sums_of[1]).astype(bf16)

    loads[4].wait()
    turn = list(range(chunks))[::-1]

    def piece_of(ref, k):
        return lambda i: ref.at[i, pl.ds(k * chunk_slots, chunk_slots)]

    def expert_down(t):
        eo_send[t] = jnp.dot(hidden_units, ed[:, columns(t)], preferred_element_type=f32).astype(bf16)

    eo_copies = [[None] * groups for k in range(chunks)]

    def expert_pair(d):
        expert_down(other(d) * 2 + 1 - parity)
        for k in turn:
            eo_copies[k][d] = scatter_pair(piece_of(eo_send, k), piece_of(eo_one, k), d)

    for d in range(1, groups):
        expert_pair(d)
    for k in range(3, chunks):
        pre_done(k)
    for d in range(1, groups):
        expert_down(ahead(d))
    expert_pair(0)
    for k in turn:
        scatter_cross(
            piece_of(eo_send, k), piece_of(eo_one, k), piece_of(eo_mid, k), piece_of(eo_two, k), eo_copies[k]
        )
    expert_down(tp)
    for k in range(chunks):
        hid_relay(k)
    loads[5].wait()
    units = hid.shape[3]
    for k in range(chunks):
        arrive(hid_copies[k][groups - 1 :])
    dense_out[...] = jnp.dot(
        hid[...].reshape(ep_count * seqs, units), dd[...], preferred_element_type=f32
    )
    for p in range(ep_count):
        rows = slice(p * seqs, (p + 1) * seqs)
        dense_out[rows] = gates[p] * dense_out[rows]
    relayed = range(chunks // 2, chunks // 2 + 1)
    c_copies = {}
    parts = {}
    near = {}
    first_dims = (((0,), (0,)), ((), ()))

    def c_cross(k):
        for p in range(k * per, (k + 1) * per, 2):
            near[p].wait_recv()
            c_send[p] = (parts[p] + c_recv[p + 1].astype(f32)).astype(bf16)
            c_copies[p] = ep_copy(c_send.at[p], c_recv.at[p], p)

    for k in turn:
        total = scatter_sum(piece_of(eo_send, k), piece_of(eo_one, k), piece_of(eo_two, k), eo_copies[k])
        total = total.astype(bf16)
        picked = lax.dot_general(placings[k], total, first_dims, preferred_element_type=f32)
        for q in list(range(per))[::-1]:
            p = k * per + q
            combined = (
                dense_out[p * seqs : (p + 1) * seqs] + shares[p] * picked[q * seqs : (q + 1) * seqs]
            )
            if p == 0:
                parts[p] = combined
            elif k in relayed and p % 2 == 0:
                parts[p] = combined
            else:
                c_send[p] = combined.astype(bf16)
                if k in relayed:
                    near[p - 1] = ep_copy(c_send.at[p], c_recv.at[p], 1)
                else:
                    c_copies[p] = ep_copy(c_send.at[p], c_recv.at[p], p)
        if k == 0:
            for late in reversed(relayed):
                c_cross(late)
    ffn = parts[0]
    for p in sorted(c_copies):
        c_copies[p].wait_recv()
        ffn = ffn + c_recv[p].astype(f32)
    fs_send[0:1, 0:seqs] = to_row(jnp.sum(ffn * ffn, axis=1, keepdims=True))
    final_copies = tp_all(lambda peer: fs_send, fs_recv.at[tp])
    scaled = gain_three * ffn
    squares = fs_send[...]
    arrive(final_copies)
    for d in range(1, tp_count):
        squares = squares + fs_recv[from_tp(d)]
    scale = to_column(lax.rsqrt(squares[0:1, 0:seqs] / width + EPS))
    out_ref[...] = (residual + scaled * scale).astype(bf16)
    for copy in started:
        copy.wait_send()


def tail(
    terms, hidden, norm_gains, dense_mix, routes, route_scores, weights
):
    tp_count = lax.axis_size("tp")
    ep_count = lax.axis_size("ep")
    seqs, width = hidden.shape
    part = width // tp_count
    expert_gate, expert_up, expert_down, dense_gate, dense_up, dense_down = weights
    units = expert_gate.shape[2]
    dense_gate, dense_up = dense_gate.T, dense_up.T
    dense_units = dense_gate.shape[0]
    top = routes.shape[1]
    experts = ep_count * expert_gate.shape[0]
    limit = 2 * seqs * top // ep_count
    capacity = -(-limit // 16) * 16
    chunks = 4
    rows_all = ep_count * seqs
    quarter = rows_all // chunks // tp_count
    groups = tp_count // 2
    lanes = -(-seqs // 128) * 128
    f32, bf16 = jnp.float32, jnp.bfloat16
    vmem = pl.BlockSpec(memory_space=pltpu.VMEM)
    hbm = pl.BlockSpec(memory_space=pl.ANY)
    slots = ep_count * capacity
    tp_copies = 3 * (tp_count - 1) + 4 * chunks * (2 * groups - 1)
    ep_copies = 4 * (ep_count - 1)
    sums = -(-6 * seqs // 128) * 128
    piece = pltpu.VMEM((chunks, groups, 2, quarter, dense_units), bf16)
    return pl.pallas_call(
        functools.partial(tail_kernel, tp_count, ep_count, capacity, chunks),
        out_shape=jax.ShapeDtypeStruct((seqs, part), bf16),
        in_specs=[hbm] * 12,
        out_specs=vmem,
        scratch_shapes=[
            pltpu.VMEM((tp_count, seqs, part), bf16),
            pltpu.VMEM((seqs, part), bf16),
            pltpu.VMEM((norm_gains.shape[0], part), f32),
            pltpu.VMEM((1, part), f32),
            pltpu.VMEM((top, seqs), jnp.int32),
            pltpu.VMEM((top, seqs), f32),
            pltpu.VMEM((width, units), bf16),
            pltpu.VMEM((width, units), bf16),
            pltpu.VMEM((units, width), bf16),
            pltpu.VMEM(dense_gate.shape, bf16),
            pltpu.VMEM(dense_up.shape, bf16),
            pltpu.VMEM(dense_down.shape, bf16),
            pltpu.VMEM(dense_gate.shape[::-1], bf16),
            pltpu.VMEM(dense_up.shape[::-1], bf16),
            pltpu.VMEM((tp_count, seqs, part), bf16),
            pltpu.VMEM((1, sums), f32),
            pltpu.VMEM((tp_count, 1, sums), f32),
            pltpu.VMEM((1, lanes), f32),
            pltpu.VMEM((tp_count, 1, lanes), f32),
            pltpu.VMEM((2, experts, lanes), f32),
            pltpu.VMEM((ep_count, 2, experts, lanes), f32),
            pltpu.VMEM((1, lanes), f32),
            pltpu.VMEM((ep_count, 1, lanes), f32),
            pltpu.VMEM((ep_count, seqs, part), bf16),
            pltpu.VMEM((tp_count, slots, part), bf16),
            pltpu.VMEM((chunks, tp_count, 2, quarter, dense_units), bf16),
            piece,
            piece,
            piece,
            pltpu.VMEM((chunks, tp_count, quarter, dense_units), bf16),
            pltpu.VMEM((rows_all, part), f32),
            pltpu.VMEM((tp_count, slots, part), bf16),
            pltpu.VMEM((groups, slots, part), bf16),
            pltpu.VMEM((groups, slots, part), bf16),
            pltpu.VMEM((groups, slots, part), bf16),
            pltpu.VMEM((ep_count, seqs, part), bf16),
            pltpu.VMEM((ep_count, seqs, part), bf16),
            pltpu.SemaphoreType.DMA((6,)),
            pltpu.SemaphoreType.DMA((6,)),
            pltpu.SemaphoreType.REGULAR,
            pltpu.SemaphoreType.REGULAR,
            pltpu.SemaphoreType.DMA((tp_copies,)),
            pltpu.SemaphoreType.DMA((tp_copies,)),
            pltpu.SemaphoreType.DMA((ep_copies,)),
            pltpu.SemaphoreType.DMA((ep_copies,)),
        ],
        compiler_params=pltpu.CompilerParams(
            collective_id=0, has_side_effects=True, vmem_limit_bytes=67043328
        ),
        name="tail",
    )(
        terms,
        hidden,
        norm_gains,
        dense_mix.reshape(1, width),
        routes.T,
        route_scores.T,
        expert_gate,
        expert_up,
        expert_down,
        dense_gate,
        dense_up,
        dense_down,
    )


def local(
    hidden,
    norm_gains,
    w_query,
    w_key,
    w_value,
    w_outgate,
    w_input_gate,
    w_forget_gate,
    forget_bias,
    w_mix_out,
    state_matrix,
    state_norm,
    state_max,
    routes,
    route_scores,
    expert_gate,
    expert_up,
    expert_down,
    dense_gate,
    dense_up,
    dense_down,
    dense_mix,
):
    terms, new_matrix, new_norm, new_max = front(
        hidden,
        norm_gains,
        (w_input_gate, w_forget_gate),
        forget_bias,
        state_norm,
        state_max,
        (w_query, w_key, w_value, w_outgate, w_mix_out),
        state_matrix,
    )
    new_hidden = tail(
        terms,
        hidden,
        norm_gains,
        dense_mix,
        routes,
        route_scores,
        (expert_gate, expert_up, expert_down, dense_gate, dense_up, dense_down),
    )
    return (new_hidden, new_matrix, new_norm, new_max)


def solution(mesh):
    placed = (
        P("ep", None),
        P(),
        P(None, "tp"),
        P(None, "tp"),
        P(None, "tp"),
        P(None, "tp"),
        P(),
        P(),
        P(),
        P("tp", None),
        P("ep", "tp", None, None),
        P("ep", "tp", None),
        P("ep", "tp"),
        P("ep", None),
        P("ep", None),
        P("ep", None, "tp"),
        P("ep", None, "tp"),
        P("ep", "tp", None),
        P("tp", "ep"),
        P("tp", "ep"),
        P("ep", "tp"),
        P(),
    )
    return jax.shard_map(
        local,
        mesh=mesh,
        in_specs=placed,
        out_specs=(P("ep", "tp"), P("ep", "tp", None, None), P("ep", "tp", None), P("ep", "tp")),
        check_vma=False,
    )
```

```python
import functools

import jax
import jax.numpy as jnp
from jax import lax
from jax.experimental import pallas as pl
from jax.experimental.pallas import tpu as pltpu
from jax.sharding import PartitionSpec as P

EPS = 1e-06


def front_kernel(
    hidden_hbm,
    gains_hbm,
    in_hbm,
    forget_hbm,
    bias_hbm,
    norm_hbm,
    max_hbm,
    wq_hbm,
    wk_hbm,
    wv_hbm,
    wo_hbm,
    wm_hbm,
    state_hbm,
    terms_hbm,
    matrix_hbm,
    new_norm_hbm,
    new_max_ref,
    wq,
    wk,
    wv,
    wo,
    wm,
    hidden,
    gains,
    in_weight,
    forget_weight,
    bias,
    norm,
    top,
    state,
    numer,
    terms,
    new_norms,
    s_sem,
    w_sem,
    in_sem,
    out_sem,
    end_sem,
):
    tp = lax.axis_index("tp")
    f32, bf16 = jnp.float32, jnp.bfloat16
    seqs = hidden.shape[0]
    heads, head = state.shape[1], state.shape[2]
    chunks = in_sem.shape[0]
    step = seqs // chunks
    smalls = []
    for i, (src, dst) in enumerate(
        (
            (hidden_hbm, hidden),
            (gains_hbm, gains),
            (in_hbm, in_weight),
            (forget_hbm, forget_weight),
            (bias_hbm, bias),
            (max_hbm, top),
            (norm_hbm, norm),
        )
    ):
        smalls.append(pltpu.make_async_copy(src, dst, s_sem.at[i]))
    for small in smalls[:4]:
        small.start()
    loads = []
    for i, (src, dst) in enumerate(((wk_hbm, wk), (wq_hbm, wq), (wv_hbm, wv), (wo_hbm, wo), (wm_hbm, wm))):
        loads.append(pltpu.make_async_copy(src, dst, w_sem.at[i]))
    fetches = []
    for c in range(chunks):
        rows = pl.ds(c * step, step)
        fetches.append(pltpu.make_async_copy(state_hbm.at[rows], state.at[rows], in_sem.at[c]))
    for load in loads[:3]:
        load.start()
    for small in smalls[4:]:
        small.start()
    for small in smalls[:4]:
        small.wait()
    for fetch in fetches:
        fetch.start()
    for load in loads[3:]:
        load.start()

    start = hidden[...].astype(f32)
    scale = lax.rsqrt(jnp.mean(start * start, axis=1, keepdims=True) + EPS)
    normed = (start * scale * gains[0:1, :]).astype(bf16)
    last = (((1,), (1,)), ((), ()))
    in_all = lax.dot_general(normed, in_weight[...], last, preferred_element_type=f32)
    forget_all = lax.dot_general(normed, forget_weight[...], last, preferred_element_type=f32)
    column = lax.broadcasted_iota(jnp.int32, in_all.shape, 1)
    here = lax.broadcasted_iota(jnp.int32, (seqs, seqs), 0)
    there = lax.broadcasted_iota(jnp.int32, (seqs, seqs), 1)
    projected = []
    for i, weight in enumerate((wk, wq, wv)):
        loads[i].wait()
        product = jnp.dot(normed, weight[...], preferred_element_type=f32)
        projected.append(product.astype(bf16).astype(f32))
    keys, query, values = projected
    for small in smalls[4:]:
        small.wait()
    forget_all = forget_all + bias[...]
    forget_all = jnp.minimum(forget_all, 0.0) - jnp.log(1.0 + jnp.exp(-jnp.abs(forget_all)))
    keeps = []
    bounds = []
    outers = []
    turns = []
    for h in range(heads):
        span = slice(h * head, (h + 1) * head)
        mine = column == tp * heads + h
        in_gate = jnp.sum(jnp.where(mine, in_all, 0.0), axis=1, keepdims=True)
        log_forget = jnp.sum(jnp.where(mine, forget_all, 0.0), axis=1, keepdims=True)
        before = jnp.sum(jnp.where(here == there, top[h : h + 1, :], 0.0), axis=1, keepdims=True)
        carried = log_forget + before
        new_max = jnp.maximum(carried, in_gate)
        keep = jnp.exp(carried - new_max)
        write = jnp.exp(in_gate - new_max) * head ** (-0.5)
        new_max_ref[h : h + 1, :] = jnp.sum(
            jnp.where(here == there, new_max, 0.0), axis=0, keepdims=True
        )
        new_norm = keep * norm[:, h, :] + write * keys[:, span]
        new_norms[:, h, :] = new_norm
        denom = jnp.sum(query[:, span] * new_norm, axis=1, keepdims=True)
        bounds.append(jnp.maximum(jnp.abs(denom), jnp.exp(-new_max)))
        keeps.append(jnp.broadcast_to(keep, (seqs, head)))
        added = write * values[:, span]
        high = added.astype(bf16).astype(f32)
        middle = (added - high).astype(bf16).astype(f32)
        low = (added - high - middle).astype(bf16).astype(f32)
        outers.append(jnp.concatenate([high, middle, low, jnp.zeros_like(low)], axis=0))
        turned = jnp.concatenate([keys[:, span]] * 3 + [query[:, span]], axis=0).T
        turns.append((turned, turned.astype(bf16)))
    norm_store = pltpu.make_async_copy(new_norms, new_norm_hbm, end_sem.at[0])
    norm_store.start()
    from_seq = lax.rem(lax.broadcasted_iota(jnp.int32, outers[0].shape, 0), seqs)
    stores = []
    for c in range(chunks):
        fetches[c].wait()
        for s in range(c * step, (c + 1) * step, 2):
            for h in range(heads):
                turned, turned_half = turns[h]
                picked = [jnp.where(from_seq == s + i, outers[h], 0.0).astype(bf16) for i in range(2)]
                written = jnp.dot(
                    turned_half, jnp.concatenate(picked, axis=1), preferred_element_type=f32
                )
                for i in range(2):
                    at = 3 * seqs + s + i
                    query_col = turned[:, at : at + 1]
                    new = (
                        keeps[h][s + i : s + i + 1, :] * state[s + i, h]
                        + written[:, i * head : (i + 1) * head]
                    )
                    state[s + i, h] = new
                    numer[h, s + i : s + i + 1, :] = jnp.sum(query_col * new, axis=0, keepdims=True)
        rows = pl.ds(c * step, step)
        stores.append(pltpu.make_async_copy(state.at[rows], matrix_hbm.at[rows], out_sem.at[c]))
        stores[c].start()
    loads[3].wait()
    gate = jnp.dot(normed, wo[...], preferred_element_type=f32).astype(bf16).astype(f32)
    mixed = []
    for h in range(heads):
        span = slice(h * head, (h + 1) * head)
        mixed.append((jax.nn.sigmoid(gate[:, span]) * (numer[h] / bounds[h])).astype(bf16))
    mixed = jnp.concatenate(mixed, axis=1)
    loads[4].wait()
    part = terms.shape[2]
    for t in range(terms.shape[0]):
        terms[t] = jnp.dot(
            mixed, wm[:, t * part : (t + 1) * part], preferred_element_type=f32
        ).astype(bf16)
    terms_store = pltpu.make_async_copy(terms, terms_hbm, end_sem.at[1])
    terms_store.start()
    for store in stores + [norm_store, terms_store]:
        store.wait()


def front(hidden, norm_gains, gate_weights, forget_bias, state_norm, state_max, weights, state_matrix):
    tp_count = lax.axis_size("tp")
    seqs, width = hidden.shape
    heads, head = state_matrix.shape[1], state_matrix.shape[2]
    f32, bf16 = jnp.float32, jnp.bfloat16
    chunks = 4
    vmem = pl.BlockSpec(memory_space=pltpu.VMEM)
    hbm = pl.BlockSpec(memory_space=pl.ANY)
    smalls = (
        hidden,
        norm_gains,
        gate_weights[0].T,
        gate_weights[1].T,
        forget_bias.reshape(1, -1),
        state_norm,
        state_max.T,
    )
    terms, matrix, norm, top = pl.pallas_call(
        front_kernel,
        out_shape=(
            jax.ShapeDtypeStruct((tp_count, seqs, width // tp_count), bf16),
            jax.ShapeDtypeStruct(state_matrix.shape, f32),
            jax.ShapeDtypeStruct(state_norm.shape, f32),
            jax.ShapeDtypeStruct((heads, seqs), f32),
        ),
        in_specs=[hbm] * 13,
        out_specs=(hbm, hbm, hbm, vmem),
        scratch_shapes=[pltpu.VMEM(weight.shape, bf16) for weight in weights]
        + [pltpu.VMEM(small.shape, small.dtype) for small in smalls]
        + [
            pltpu.VMEM(state_matrix.shape, f32),
            pltpu.VMEM((heads, seqs, head), f32),
            pltpu.VMEM((tp_count, seqs, width // tp_count), bf16),
            pltpu.VMEM(state_norm.shape, f32),
            pltpu.SemaphoreType.DMA((7,)),
            pltpu.SemaphoreType.DMA((5,)),
            pltpu.SemaphoreType.DMA((chunks,)),
            pltpu.SemaphoreType.DMA((chunks,)),
            pltpu.SemaphoreType.DMA((2,)),
        ],
        compiler_params=pltpu.CompilerParams(vmem_limit_bytes=67043328),
        name="front",
    )(*smalls, *weights, state_matrix)
    return terms, matrix, norm, top.T


MESH = pl.DeviceIdType.MESH


def tail_kernel(
    tp_count,
    ep_count,
    capacity,
    chunks,
    terms_hbm,
    hidden_hbm,
    gains_hbm,
    mix_hbm,
    routes_hbm,
    scores_hbm,
    eg_hbm,
    eu_hbm,
    ed_hbm,
    dg_hbm,
    du_hbm,
    dd_hbm,
    out_ref,
    terms,
    start_in,
    gains,
    mix,
    routes,
    scores,
    eg,
    eu,
    ed,
    dg,
    du,
    dd,
    dgt,
    dut,
    br_recv,
    st_send,
    st_recv,
    fs_send,
    fs_recv,
    info_send,
    info_recv,
    mg_send,
    mg_recv,
    rows_in,
    xin,
    pre_send,
    pre_one,
    pre_mid,
    pre_two,
    hid,
    dense_out,
    eo_send,
    eo_one,
    eo_mid,
    eo_two,
    c_send,
    c_recv,
    s_sem,
    w_sem,
    join_sem,
    go_sem,
    tp_send,
    tp_recv,
    ep_send,
    ep_recv,
):
    tp = lax.axis_index("tp")
    ep = lax.axis_index("ep")
    seqs, part = start_in.shape
    width = part * tp_count
    per = ep_count // chunks
    chunk_rows = per * seqs
    chunk_slots = per * capacity
    quarter = chunk_rows // tp_count
    first = pl.multiple_of(tp * part, part)
    f32, bf16 = jnp.float32, jnp.bfloat16

    own = pl.ds(first, part)
    smalls = []
    for i, (src, dst) in enumerate(
        (
            (terms_hbm, terms),
            (hidden_hbm.at[:, own], start_in),
            (gains_hbm.at[:, own], gains),
            (mix_hbm.at[:, own], mix),
            (routes_hbm, routes),
            (scores_hbm, scores),
        )
    ):
        load = pltpu.make_async_copy(src, dst, s_sem.at[i])
        load.start()
        smalls.append(load)

    def partner(p):
        other = ep
        bit = 1
        while bit < ep_count:
            if p & bit:
                other = other + bit * (1 - 2 * lax.rem(ep // bit, 2))
            bit *= 2
        return other

    barrier = pltpu.get_barrier_semaphore()
    for d in range(1, tp_count):
        peer = lax.rem(tp + d, tp_count)

        @pl.when(peer != 0)
        def _(peer=peer):
            pl.semaphore_signal(barrier, inc=1, device_id={"tp": peer}, device_id_type=MESH)

    loads = []
    for i, (src, dst) in enumerate(
        ((dg_hbm, dg), (du_hbm, du), (eg_hbm.at[0], eg), (eu_hbm.at[0], eu), (ed_hbm.at[0], ed), (dd_hbm, dd))
    ):
        load = pltpu.make_async_copy(src, dst, w_sem.at[i])
        load.start()
        loads.append(load)

    groups = tp_count // 2
    parity = lax.rem(tp, 2)
    group = tp // 2
    pair = tp + 1 - 2 * parity
    started = []
    tp_next = [0]
    ep_next = [0]

    def tp_copy(src, dst, peer):
        at = tp_next[0]
        tp_next[0] += 1
        copy = pltpu.make_async_remote_copy(
            src_ref=src,
            dst_ref=dst,
            send_sem=tp_send.at[at],
            recv_sem=tp_recv.at[at],
            device_id={"tp": peer},
            device_id_type=MESH,
        )
        copy.start()
        started.append(copy)
        return copy

    def ep_copy(src, dst, p):
        at = ep_next[0]
        ep_next[0] += 1
        copy = pltpu.make_async_remote_copy(
            src_ref=src,
            dst_ref=dst,
            send_sem=ep_send.at[at],
            recv_sem=ep_recv.at[at],
            device_id={"ep": partner(p)},
            device_id_type=MESH,
        )
        copy.start()
        started.append(copy)
        return copy

    def tp_all(src_of, dst):
        made = []
        for d in range(1, tp_count):
            peer = lax.rem(tp + d, tp_count)
            made.append(tp_copy(src_of(peer), dst, peer))
        return made

    def ahead(d):
        return lax.rem(group + d, groups) * 2 + parity

    def behind(d):
        return lax.rem(group + groups - d, groups) * 2 + parity

    def gather_start(at):
        made = [tp_copy(at(tp), at(tp), ahead(d)) for d in range(1, groups)]
        made.append(tp_copy(at(tp), at(tp), pair))
        return made

    def gather_relay(at, made):
        for d in range(1, groups):
            made[d - 1].wait_recv()
            made.append(tp_copy(at(behind(d)), at(behind(d)), pair))

    def other(d):
        return lax.rem(group + d, groups)

    def scatter_pair(at, one, d):
        return tp_copy(at(other(d) * 2 + 1 - parity), one(other(d)), pair)

    def scatter_cross(at, one, mid, two, made):
        for d in range(1, groups):
            j = other(d)
            made[d].wait_recv()
            mid(j)[...] = (at(ahead(d))[...].astype(f32) + one(j)[...].astype(f32)).astype(bf16)
            made.append(tp_copy(mid(j), two(group), ahead(d)))

    def scatter_sum(at, one, two, made):
        made[0].wait_recv()
        total = at(tp)[...].astype(f32) + one(group)[...].astype(f32)
        for d in range(1, groups):
            made[groups + d - 1].wait_recv()
            total = total + two(lax.rem(group + groups - d, groups))[...].astype(f32)
        return total

    def arrive(copies):
        for copy in copies:
            copy.wait_recv()

    def from_tp(d):
        return lax.rem(tp + tp_count - d, tp_count)

    def columns(peer):
        return pl.ds(pl.multiple_of(peer * part, part), part)

    for ref in (fs_send, mg_send, info_send):
        ref[...] = jnp.zeros(ref.shape, f32)
    here = lax.broadcasted_iota(jnp.int32, (seqs, seqs), 0)
    there = lax.broadcasted_iota(jnp.int32, (seqs, seqs), 1)
    diagonal = here == there

    def to_row(column):
        return jnp.sum(jnp.where(diagonal, column, 0.0), axis=0, keepdims=True)

    def to_column(row):
        return jnp.sum(jnp.where(diagonal, row, 0.0), axis=1, keepdims=True)


    @pl.when(tp != 0)
    def _():
        pl.semaphore_wait(barrier, tp_count - 1)
        pl.semaphore_signal(join_sem, inc=1, device_id={"tp": 0}, device_id_type=MESH)

    @pl.when(tp == 0)
    def _():
        pl.semaphore_wait(join_sem, tp_count - 1)
        for p in range(1, ep_count):
            pl.semaphore_signal(barrier, inc=1, device_id={"ep": partner(p)}, device_id_type=MESH)

    for load in smalls:
        load.wait()
    branch_copies = tp_all(lambda peer: terms.at[peer], br_recv.at[tp])

    top = routes.shape[0]
    experts = info_send.shape[0]
    name = lax.broadcasted_iota(jnp.int32, (experts, seqs), 0)
    hits = [routes[k : k + 1, :] == name for k in range(top)]
    named = hits[0]
    for k in range(1, top):
        named = jnp.logical_or(named, hits[k])
    named = jnp.where(named, 1.0, 0.0)
    before = jnp.where(here < there, 1.0, 0.0).astype(bf16)
    rank = jnp.dot(named.astype(bf16), before, preferred_element_type=f32) + 1.0
    score_sum = scores[0:1, :]
    for k in range(1, top):
        score_sum = score_sum + scores[k : k + 1, :]
    share = jnp.zeros((experts, seqs), f32)
    for k in range(top):
        share = share + jnp.where(hits[k], scores[k : k + 1, :] / score_sum, 0.0)
    info_send[:, 0 : 2 * seqs] = jnp.concatenate([named * rank, share], axis=1)

    start_part = start_in[...].astype(f32)
    gain_one = gains[1:2, :]
    gain_two = gains[2:3, :]
    gain_three = gains[3:4, :]
    mix_weight = gain_two * mix[...]
    start_sq = jnp.sum(start_part * start_part, axis=1, keepdims=True)
    start_dot = jnp.sum(start_part * mix_weight, axis=1, keepdims=True)
    branch = terms[tp].astype(f32)
    loads[0].wait()
    dgt[...] = dg[...].T
    arrive(branch_copies)
    for d in range(1, tp_count):
        branch = branch + br_recv[from_tp(d)].astype(f32)
    branch = branch.astype(bf16).astype(f32)
    lifted = gain_one * branch
    lanes = st_send.shape[1]
    lane = lax.broadcasted_iota(jnp.int32, (seqs, lanes), 1)
    place_of = lax.broadcasted_iota(jnp.int32, (seqs, lanes), 0)

    def pack(values):
        made = jnp.zeros((seqs, lanes), f32)
        for i, value in enumerate(values):
            made = jnp.where(lane == place_of + i * seqs, value, made)
        return jnp.sum(made, axis=0, keepdims=True)

    def unpack(row, i):
        return jnp.sum(jnp.where(lane == place_of + i * seqs, row, 0.0), axis=1, keepdims=True)

    packed = pack(
        (
            jnp.sum(branch * branch, axis=1, keepdims=True),
            start_sq,
            jnp.sum(start_part * lifted, axis=1, keepdims=True),
            jnp.sum(lifted * lifted, axis=1, keepdims=True),
            start_dot,
            jnp.sum(lifted * mix_weight, axis=1, keepdims=True),
        )
    )
    st_send[...] = packed
    stat_copies = tp_all(lambda peer: st_send, st_recv.at[tp])

    @pl.when(tp == 0)
    def _():
        pl.semaphore_wait(barrier, ep_count - 1)
        for t in range(1, tp_count):
            pl.semaphore_signal(go_sem, inc=1, device_id={"tp": t}, device_id_type=MESH)

    @pl.when(tp != 0)
    def _():
        pl.semaphore_wait(go_sem, 1)

    info_copies = [ep_copy(info_send, info_recv.at[p], p) for p in range(1, ep_count)]
    loads[1].wait()
    dut[...] = du[...].T
    arrive(stat_copies)
    for d in range(1, tp_count):
        packed = packed + st_recv[from_tp(d)]
    branch_sq, start_sq, cross_sum, lifted_sq, start_dot, lifted_dot = (
        unpack(packed, i) for i in range(6)
    )
    branch_scale = lax.rsqrt(branch_sq / width + EPS)
    resid_sq = start_sq + 2.0 * branch_scale * cross_sum + branch_scale * branch_scale * lifted_sq
    gate_dot = start_dot + branch_scale * lifted_dot
    scale_two = lax.rsqrt(resid_sq / width + EPS)
    residual_f = start_part + lifted * branch_scale
    residual = residual_f.astype(bf16).astype(f32)
    rows_in[0] = (residual_f * scale_two * gain_two).astype(bf16)
    row_copies = [None] * ep_count
    for p in list(range(1, ep_count)):
        row_copies[p] = ep_copy(rows_in.at[0], rows_in.at[p], p)
    mix_gate = jax.nn.sigmoid(scale_two * gate_dot)
    mg_send[0:1, 0:seqs] = to_row(mix_gate)
    mg_copies = [ep_copy(mg_send, mg_recv.at[p], p) for p in range(1, ep_count)]
    mine = lax.broadcasted_iota(jnp.int32, info_send.shape, 0) == ep
    info_lane = lax.broadcasted_iota(jnp.int32, (seqs, info_send.shape[1]), 1)
    info_seq = lax.broadcasted_iota(jnp.int32, (seqs, info_send.shape[1]), 0)
    wanted = (lax.broadcasted_iota(jnp.int32, (capacity, seqs), 0) + 1).astype(f32)
    wide_row = lax.broadcasted_iota(jnp.int32, (seqs, chunk_rows), 0)
    wide_column = lax.broadcasted_iota(jnp.int32, (seqs, chunk_rows), 1)
    arrive(info_copies)
    placings = []
    shares = []
    for k in range(chunks):
        blocks = []
        for q in range(per):
            p = k * per + q
            info = info_send[...] if p == 0 else info_recv[p]
            info = jnp.sum(jnp.where(mine, info, 0.0), axis=0, keepdims=True)
            one = jnp.where(info[:, 0:seqs] == wanted, 1.0, 0.0).astype(bf16)
            moved = jnp.where(wide_row + q * seqs == wide_column, 1.0, 0.0).astype(bf16)
            blocks.append(jnp.dot(one, moved, preferred_element_type=f32).astype(bf16))
            shares.append(
                jnp.sum(jnp.where(info_lane == info_seq + seqs, info, 0.0), axis=1, keepdims=True)
            )
        placings.append(jnp.concatenate(blocks, axis=0))

    def xin_at(k):
        return lambda i: xin.at[i, pl.ds(k * chunk_slots, chunk_slots)]

    def pre_at(k):
        return lambda i: pre_send.at[k, i]

    def of(ref, k):
        return lambda j: ref.at[k, j]

    def hid_at(k):
        return lambda i: hid.at[k, i]

    xin_copies = []
    pre_copies = []
    hid_copies = []

    def chunk_in(k):
        for p in range(k * per, (k + 1) * per):
            if p > 0:
                row_copies[p].wait_recv()
        rows = rows_in[k * per : (k + 1) * per].reshape(chunk_rows, part)
        xin[tp, k * chunk_slots : (k + 1) * chunk_slots] = jnp.dot(
            placings[k], rows, preferred_element_type=f32
        ).astype(bf16)
        xin_copies.append(gather_start(xin_at(k)))
        for i, weight in enumerate((dgt, dut)):
            made = jnp.dot(rows, weight[...], preferred_element_type=f32).astype(bf16)
            for t in range(tp_count):
                pre_send[k, t, i] = made[t * quarter : (t + 1) * quarter]
        far_first = list(range(1, groups)) + [0]
        made = {d: scatter_pair(pre_at(k), of(pre_one, k), d) for d in far_first}
        pre_copies.append([made[d] for d in range(groups)])

    def pre_cross(k):
        scatter_cross(pre_at(k), of(pre_one, k), of(pre_mid, k), of(pre_two, k), pre_copies[k])

    def pre_done(k):
        pre = scatter_sum(pre_at(k), of(pre_one, k), of(pre_two, k), pre_copies[k])
        hid[k, tp] = (jax.nn.silu(pre[0]) * pre[1]).astype(bf16)
        hid_copies.append(gather_start(hid_at(k)))

    def xin_relay(k):
        gather_relay(xin_at(k), xin_copies[k])

    def hid_relay(k):
        gather_relay(hid_at(k), hid_copies[k])

    sums_of = [None, None]

    def expert_in(source):
        for i, weight in enumerate((eg, eu)):
            made = jnp.dot(xin[source], weight[columns(source), :], preferred_element_type=f32)
            sums_of[i] = made if sums_of[i] is None else sums_of[i] + made

    chunk_in(0)
    pre_cross(0)
    for k in range(1, chunks):
        chunk_in(k)
        if k >= 2:
            pre_cross(k - 1)
    arrive(mg_copies)
    gates = [mix_gate] + [to_column(mg_recv[p, 0:1, 0:seqs]) for p in range(1, ep_count)]
    loads[2].wait()
    loads[3].wait()
    expert_in(tp)
    pre_cross(chunks - 1)
    for k in range(chunks - 1):
        xin_relay(k)
    pre_done(0)
    for k in range(chunks):
        xin_copies[k][groups - 1].wait_recv()
    expert_in(pair)
    xin_relay(chunks - 1)
    pre_done(1)
    for d in range(1, groups):
        expert_in(behind(d))
    pre_done(2)
    for d in range(1, groups):
        for k in range(chunks):
            xin_copies[k][groups - 1 + d].wait_recv()
        expert_in(behind(d) + 1 - 2 * parity)
    hidden_units = (jax.nn.silu(sums_of[0]) * sums_of[1]).astype(bf16)

    loads[4].wait()
    turn = list(range(chunks))[::-1]

    def piece_of(ref, k):
        return lambda i: ref.at[i, pl.ds(k * chunk_slots, chunk_slots)]

    def expert_down(t):
        eo_send[t] = jnp.dot(hidden_units, ed[:, columns(t)], preferred_element_type=f32).astype(bf16)

    eo_copies = [[None] * groups for k in range(chunks)]

    def expert_pair(d):
        expert_down(other(d) * 2 + 1 - parity)
        for k in turn:
            eo_copies[k][d] = scatter_pair(piece_of(eo_send, k), piece_of(eo_one, k), d)

    for d in range(1, groups):
        expert_pair(d)
    for k in range(3, chunks):
        pre_done(k)
    for d in range(1, groups):
        expert_down(ahead(d))
    expert_pair(0)
    for k in turn:
        scatter_cross(
            piece_of(eo_send, k), piece_of(eo_one, k), piece_of(eo_mid, k), piece_of(eo_two, k), eo_copies[k]
        )
    expert_down(tp)
    for k in range(chunks):
        hid_relay(k)
    loads[5].wait()
    units = hid.shape[3]
    for k in range(chunks):
        arrive(hid_copies[k][groups - 1 :])
    dense_out[...] = jnp.dot(
        hid[...].reshape(ep_count * seqs, units), dd[...], preferred_element_type=f32
    )
    for p in range(ep_count):
        rows = slice(p * seqs, (p + 1) * seqs)
        dense_out[rows] = gates[p] * dense_out[rows]
    relayed = range(chunks // 2, chunks // 2 + 1)
    c_copies = {}
    parts = {}
    near = {}
    first_dims = (((0,), (0,)), ((), ()))

    def c_cross(k):
        for p in range(k * per, (k + 1) * per, 2):
            near[p].wait_recv()
            c_send[p] = (parts[p] + c_recv[p + 1].astype(f32)).astype(bf16)
            c_copies[p] = ep_copy(c_send.at[p], c_recv.at[p], p)

    for k in turn:
        total = scatter_sum(piece_of(eo_send, k), piece_of(eo_one, k), piece_of(eo_two, k), eo_copies[k])
        total = total.astype(bf16)
        picked = lax.dot_general(placings[k], total, first_dims, preferred_element_type=f32)
        for q in list(range(per))[::-1]:
            p = k * per + q
            combined = (
                dense_out[p * seqs : (p + 1) * seqs] + shares[p] * picked[q * seqs : (q + 1) * seqs]
            )
            if p == 0:
                parts[p] = combined
            elif k in relayed and p % 2 == 0:
                parts[p] = combined
            else:
                c_send[p] = combined.astype(bf16)
                if k in relayed:
                    near[p - 1] = ep_copy(c_send.at[p], c_recv.at[p], 1)
                else:
                    c_copies[p] = ep_copy(c_send.at[p], c_recv.at[p], p)
        if k == 0:
            for late in reversed(relayed):
                c_cross(late)
    ffn = parts[0]
    for p in sorted(c_copies):
        c_copies[p].wait_recv()
        ffn = ffn + c_recv[p].astype(f32)
    fs_send[0:1, 0:seqs] = to_row(jnp.sum(ffn * ffn, axis=1, keepdims=True))
    final_copies = tp_all(lambda peer: fs_send, fs_recv.at[tp])
    scaled = gain_three * ffn
    squares = fs_send[...]
    arrive(final_copies)
    for d in range(1, tp_count):
        squares = squares + fs_recv[from_tp(d)]
    scale = to_column(lax.rsqrt(squares[0:1, 0:seqs] / width + EPS))
    out_ref[...] = (residual + scaled * scale).astype(bf16)
    for copy in started:
        copy.wait_send()


def tail(
    terms, hidden, norm_gains, dense_mix, routes, route_scores, weights
):
    tp_count = lax.axis_size("tp")
    ep_count = lax.axis_size("ep")
    seqs, width = hidden.shape
    part = width // tp_count
    expert_gate, expert_up, expert_down, dense_gate, dense_up, dense_down = weights
    units = expert_gate.shape[2]
    dense_gate, dense_up = dense_gate.T, dense_up.T
    dense_units = dense_gate.shape[0]
    top = routes.shape[1]
    experts = ep_count * expert_gate.shape[0]
    limit = 2 * seqs * top // ep_count
    capacity = -(-limit // 16) * 16
    chunks = 4
    rows_all = ep_count * seqs
    quarter = rows_all // chunks // tp_count
    groups = tp_count // 2
    lanes = -(-seqs // 128) * 128
    pairs = -(-2 * seqs // 128) * 128
    f32, bf16 = jnp.float32, jnp.bfloat16
    vmem = pl.BlockSpec(memory_space=pltpu.VMEM)
    hbm = pl.BlockSpec(memory_space=pl.ANY)
    slots = ep_count * capacity
    tp_copies = 3 * (tp_count - 1) + 4 * chunks * (2 * groups - 1)
    ep_copies = 4 * (ep_count - 1)
    sums = -(-6 * seqs // 128) * 128
    piece = pltpu.VMEM((chunks, groups, 2, quarter, dense_units), bf16)
    return pl.pallas_call(
        functools.partial(tail_kernel, tp_count, ep_count, capacity, chunks),
        out_shape=jax.ShapeDtypeStruct((seqs, part), bf16),
        in_specs=[hbm] * 12,
        out_specs=vmem,
        scratch_shapes=[
            pltpu.VMEM((tp_count, seqs, part), bf16),
            pltpu.VMEM((seqs, part), bf16),
            pltpu.VMEM((norm_gains.shape[0], part), f32),
            pltpu.VMEM((1, part), f32),
            pltpu.VMEM((top, seqs), jnp.int32),
            pltpu.VMEM((top, seqs), f32),
            pltpu.VMEM((width, units), bf16),
            pltpu.VMEM((width, units), bf16),
            pltpu.VMEM((units, width), bf16),
            pltpu.VMEM(dense_gate.shape, bf16),
            pltpu.VMEM(dense_up.shape, bf16),
            pltpu.VMEM(dense_down.shape, bf16),
            pltpu.VMEM(dense_gate.shape[::-1], bf16),
            pltpu.VMEM(dense_up.shape[::-1], bf16),
            pltpu.VMEM((tp_count, seqs, part), bf16),
            pltpu.VMEM((1, sums), f32),
            pltpu.VMEM((tp_count, 1, sums), f32),
            pltpu.VMEM((1, lanes), f32),
            pltpu.VMEM((tp_count, 1, lanes), f32),
            pltpu.VMEM((experts, pairs), f32),
            pltpu.VMEM((ep_count, experts, pairs), f32),
            pltpu.VMEM((1, lanes), f32),
            pltpu.VMEM((ep_count, 1, lanes), f32),
            pltpu.VMEM((ep_count, seqs, part), bf16),
            pltpu.VMEM((tp_count, slots, part), bf16),
            pltpu.VMEM((chunks, tp_count, 2, quarter, dense_units), bf16),
            piece,
            piece,
            piece,
            pltpu.VMEM((chunks, tp_count, quarter, dense_units), bf16),
            pltpu.VMEM((rows_all, part), f32),
            pltpu.VMEM((tp_count, slots, part), bf16),
            pltpu.VMEM((groups, slots, part), bf16),
            pltpu.VMEM((groups, slots, part), bf16),
            pltpu.VMEM((groups, slots, part), bf16),
            pltpu.VMEM((ep_count, seqs, part), bf16),
            pltpu.VMEM((ep_count, seqs, part), bf16),
            pltpu.SemaphoreType.DMA((6,)),
            pltpu.SemaphoreType.DMA((6,)),
            pltpu.SemaphoreType.REGULAR,
            pltpu.SemaphoreType.REGULAR,
            pltpu.SemaphoreType.DMA((tp_copies,)),
            pltpu.SemaphoreType.DMA((tp_copies,)),
            pltpu.SemaphoreType.DMA((ep_copies,)),
            pltpu.SemaphoreType.DMA((ep_copies,)),
        ],
        compiler_params=pltpu.CompilerParams(
            collective_id=0, has_side_effects=True, vmem_limit_bytes=67043328
        ),
        name="tail",
    )(
        terms,
        hidden,
        norm_gains,
        dense_mix.reshape(1, width),
        routes.T,
        route_scores.T,
        expert_gate,
        expert_up,
        expert_down,
        dense_gate,
        dense_up,
        dense_down,
    )


def local(
    hidden,
    norm_gains,
    w_query,
    w_key,
    w_value,
    w_outgate,
    w_input_gate,
    w_forget_gate,
    forget_bias,
    w_mix_out,
    state_matrix,
    state_norm,
    state_max,
    routes,
    route_scores,
    expert_gate,
    expert_up,
    expert_down,
    dense_gate,
    dense_up,
    dense_down,
    dense_mix,
):
    terms, new_matrix, new_norm, new_max = front(
        hidden,
        norm_gains,
        (w_input_gate, w_forget_gate),
        forget_bias,
        state_norm,
        state_max,
        (w_query, w_key, w_value, w_outgate, w_mix_out),
        state_matrix,
    )
    new_hidden = tail(
        terms,
        hidden,
        norm_gains,
        dense_mix,
        routes,
        route_scores,
        (expert_gate, expert_up, expert_down, dense_gate, dense_up, dense_down),
    )
    return (new_hidden, new_matrix, new_norm, new_max)


def solution(mesh):
    placed = (
        P("ep", None),
        P(),
        P(None, "tp"),
        P(None, "tp"),
        P(None, "tp"),
        P(None, "tp"),
        P(),
        P(),
        P(),
        P("tp", None),
        P("ep", "tp", None, None),
        P("ep", "tp", None),
        P("ep", "tp"),
        P("ep", None),
        P("ep", None),
        P("ep", None, "tp"),
        P("ep", None, "tp"),
        P("ep", "tp", None),
        P("tp", "ep"),
        P("tp", "ep"),
        P("ep", "tp"),
        P(),
    )
    return jax.shard_map(
        local,
        mesh=mesh,
        in_specs=placed,
        out_specs=(P("ep", "tp"), P("ep", "tp", None, None), P("ep", "tp", None), P("ep", "tp")),
        check_vma=False,
    )
```
